128 devices in a mesh: sp: 32 (over z, y, core), tp: 4 (over x).
Axes of the slice: x: 4, y: 4, z: 4, core: 2. Of those that a mesh axis runs over, the one named last changes fastest.
Arguments:
- tokens: bfloat16 [8192, 4096], P(('sp', 'tp')), may hold values from -700 to 700
- down_query: bfloat16 [4096, 1024], replicated, may hold values from -0.09375 to 0.09375
- down_latent: bfloat16 [4096, 512], replicated, may hold values from -0.09375 to 0.09375
- down_rotary: bfloat16 [4096, 64], replicated, may hold values from -0.09375 to 0.09375
- query_gain: float32 [1024], replicated, may hold values from 0.1 to 1.9
- latent_gain: float32 [512], replicated, may hold values from 0.1 to 1.9
- up_query: bfloat16 [1024, 2048], P(None, 'tp'), may hold values from -0.1875 to 0.1875
- up_query_rotary: bfloat16 [1024, 1024], P(None, 'tp'), may hold values from -0.1875 to 0.1875
- up_key: bfloat16 [512, 2048], P(None, 'tp'), may hold values from -0.25 to 0.25
- up_value: bfloat16 [512, 2048], P(None, 'tp'), may hold values from -0.25 to 0.25
- out_weight: bfloat16 [2048, 4096], P('tp'), may hold values from -0.39648438 to 0.39648438
Outputs:
- mixed: bfloat16 [8192, 4096], P(('sp', 'tp'))
The draws below stay inside these ranges and needn't reach their ends.
All inputs are finite; a program needn't handle non-finite values.
Results may differ from the reference program's by a relative error of at most 0.03.
Values may be sent and summed in bfloat16 or wider, within the bound.
A program may use at most 192 MiB of HBM per device.

```python
import jax
import jax.numpy as jnp
from jax import lax

D = 4096
HEADS = 16
NOPE = 128
ROPE = 64
VDIM = 128
QRANK = 1024
KVRANK = 512
TOK_DEV = 256
TOKENS = 8192
N_TP = 4


def draw_tokens(key, part):
    first_key, second_key, third_key = jax.random.split(jax.random.fold_in(key, 11), 3)
    offsets = jax.random.normal(second_key, (TOKENS // TOK_DEV, D), jnp.float32) * 0.7
    shifted = jnp.repeat(offsets, TOK_DEV, axis=0)
    rough = jax.random.normal(first_key, (TOKENS, D), jnp.float32) + shifted
    return jnp.clip(rough, -700.0, 700.0).astype(jnp.bfloat16)


def shard_levels(stream_key, dims, cuts, smallest, high):
    loudness, own = 1.0, jax.random.fold_in(stream_key, 6)
    for dim, parts in cuts:
        heights = jnp.exp(jax.random.uniform(jax.random.fold_in(own, dim), (parts,), jnp.float32, smallest / len(cuts), high / len(cuts)))
        loudness = loudness * jnp.repeat(heights, dims[dim] // parts).reshape([-1 if axis == dim else 1 for axis in range(len(dims))])
    return loudness


def normal_values(rng, shape, width, bound, pieces=(), held_as=jnp.bfloat16):
    values = jax.random.normal(rng, shape, jnp.float32) * width
    if len(pieces) > 0:
        values = shard_levels(rng, shape, pieces, -0.22, 0.18) * values
    return jnp.clip(values, min=-bound, max=bound).astype(held_as)


def setup_inputs(seed: int = 0) -> dict:
    splits = jax.random.split(jax.random.key(seed), 12)
    tokens = draw_tokens(jax.random.fold_in(splits[11], 71), 0)
    down_query = normal_values(splits[1], (D, QRANK), D ** -0.5, 0.09375)
    down_latent = normal_values(splits[2], (D, KVRANK), D ** -0.5, 0.09375)
    down_rotary = normal_values(splits[3], (D, ROPE), D ** -0.5, 0.09375)
    query_gain = jnp.clip(1.0 + 0.18 * jax.random.normal(splits[4], (QRANK,), jnp.float32), 0.1, 1.9)
    latent_gain = jnp.clip(1.0 + 0.18 * jax.random.normal(splits[5], (KVRANK,), jnp.float32), 0.1, 1.9)
    up_query = normal_values(splits[6], (QRANK, HEADS * NOPE), QRANK ** -0.5, 0.1875, ((1, 4),))
    up_query_rotary = normal_values(splits[7], (QRANK, HEADS * ROPE), QRANK ** -0.5, 0.1875, ((1, 4),))
    up_key = normal_values(splits[8], (KVRANK, HEADS * NOPE), KVRANK ** -0.5, 0.25, ((1, 4),))
    up_value = normal_values(splits[9], (KVRANK, HEADS * VDIM), KVRANK ** -0.5, 0.25, ((1, 4),))
    out_weight = normal_values(splits[10], (HEADS * VDIM, D), (3.0 * (HEADS * VDIM) ** -0.5), 0.39648438, ((0, 4),))
    return dict(tokens=tokens, down_query=down_query, down_latent=down_latent, down_rotary=down_rotary, query_gain=query_gain, latent_gain=latent_gain, up_query=up_query, up_query_rotary=up_query_rotary, up_key=up_key, up_value=up_value, out_weight=out_weight)


rope_base = 500000.0
norm_eps = 1e-06
masked_score = -1e+30

def rotate_half(values, positions):
    half = values.shape[-1] // 2
    inverse = rope_base ** (-jnp.arange(0, 2 * half, 2, dtype=jnp.float32) / (2 * half))
    angles = positions.astype(jnp.float32)[:, None] * inverse
    if values.ndim == 3:
        angles = angles[:, None, :]
    cosine = jnp.cos(angles)
    sine = jnp.sin(angles)
    first = values[..., :half]
    second = values[..., half:]
    return jnp.concatenate([first * cosine - second * sine, second * cosine + first * sine], axis=-1)

def norm_rows(values, gain):
    return values * lax.rsqrt(lax.optimization_barrier(jnp.mean(values * values, axis=-1, keepdims=True)) + norm_eps) * gain

def reference(tokens, down_query, down_latent, down_rotary, query_gain, latent_gain, up_query, up_query_rotary, up_key, up_value, out_weight):
    positions = jnp.arange(TOKENS, dtype=jnp.int32)
    query_latent = norm_rows(jnp.dot(tokens, down_query, preferred_element_type=jnp.float32), query_gain).astype(jnp.bfloat16)
    kv_latent = norm_rows(jnp.dot(tokens, down_latent, preferred_element_type=jnp.float32), latent_gain).astype(jnp.bfloat16)
    key_rotary = rotate_half(jnp.dot(tokens, down_rotary, preferred_element_type=jnp.float32), positions).astype(jnp.bfloat16)
    query_plain = jnp.dot(query_latent, up_query, preferred_element_type=jnp.float32).astype(jnp.bfloat16).reshape(TOKENS, HEADS, NOPE)
    query_turned = rotate_half(jnp.dot(query_latent, up_query_rotary, preferred_element_type=jnp.float32).reshape(TOKENS, HEADS, ROPE), positions).astype(jnp.bfloat16)
    key_plain = jnp.dot(kv_latent, up_key, preferred_element_type=jnp.float32).astype(jnp.bfloat16).reshape(TOKENS, HEADS, NOPE)
    values = jnp.dot(kv_latent, up_value, preferred_element_type=jnp.float32).astype(jnp.bfloat16).reshape(TOKENS, HEADS, VDIM)
    factor = (NOPE + ROPE) ** (-0.5)
    block = 512 if TOKENS % 512 == 0 else TOKENS
    outputs = []
    for first in range(0, TOKENS, block):
        stop = first + block
        scores = jnp.einsum('qhd,khd->hqk', query_plain[first:stop].astype(jnp.float32), key_plain[:stop].astype(jnp.float32))
        scores = scores + jnp.einsum('qhr,kr->hqk', query_turned[first:stop].astype(jnp.float32), key_rotary[:stop].astype(jnp.float32))
        scores = scores * factor
        allowed = (positions[:stop][None, :] <= positions[first:stop][:, None])[None]
        scores = jnp.where(allowed, scores, masked_score)
        best = lax.optimization_barrier(jnp.max(scores, axis=-1, keepdims=True))
        weights = jnp.where(allowed, jnp.exp(scores - best), 0.0)
        total = lax.optimization_barrier(jnp.sum(weights, axis=-1))
        rounded = lax.optimization_barrier(weights.astype(jnp.bfloat16)).astype(jnp.float32)
        summed = jnp.einsum('hqk,khd->qhd', rounded, values[:stop].astype(jnp.float32))
        outputs.append((summed / jnp.transpose(total)[:, :, None]).astype(jnp.bfloat16).reshape(block, HEADS * VDIM))
    attended = jnp.concatenate(outputs, axis=0)
    group_width = HEADS * VDIM // N_TP
    mixed = jnp.zeros((TOKENS, D), jnp.float32)
    for group in range(N_TP):
        lower = group * group_width
        partial_sum = jnp.dot(attended[:, lower:lower + group_width], out_weight[lower:lower + group_width], preferred_element_type=jnp.float32)
        mixed = mixed + lax.optimization_barrier(partial_sum.astype(jnp.bfloat16)).astype(jnp.float32)
    return mixed.astype(jnp.bfloat16)
```

```python
import functools

import jax
import jax.numpy as jnp
import numpy as np
from jax import lax
from jax.experimental import pallas as pl
from jax.experimental.pallas import tpu as pltpu
from jax.sharding import PartitionSpec as P

NOPE = 128
ROPE = 64
VDIM = 128
LANES = 128

rope_base = 500000.0
norm_eps = 1e-06
masked_score = -1e30
log2e = 1.4426950408889634

EVENTS = [
    (0, 0), (3, 0), (1, 0), (0, 3), (0, 1), (2, 0), (3, 3), (1, 3),
    (3, 1), (1, 1), (0, 2), (2, 3), (2, 1), (3, 2), (1, 2), (2, 2),
]
AHEAD = 2

MESH = pl.DeviceIdType.MESH
F32 = jnp.float32
BF16 = jnp.bfloat16


def dot(a, b):
    return jnp.dot(a, b, preferred_element_type=F32)


def dot_nt(a, b):
    return lax.dot_general(a, b, (((1,), (1,)), ((), ())), preferred_element_type=F32)


def turn(v, cosine, sine):
    lane = lax.broadcasted_iota(jnp.int32, v.shape, 1)
    other = jnp.where(lane % ROPE < ROPE // 2, pltpu.roll(v, LANES - ROPE // 2, 1), pltpu.roll(v, ROPE // 2, 1))
    return v * cosine + other * sine


def normed(v, gain):
    return v * lax.rsqrt(jnp.mean(v * v, axis=-1, keepdims=True) + norm_eps) * gain


def kernel(
    S,
    T,
    chunks,
    pieces,
    tokens_hbm,
    dq_hbm,
    dl_hbm,
    dr_hbm,
    qg_ref,
    lg_ref,
    uq_hbm,
    ur_hbm,
    uk_hbm,
    uv_hbm,
    ow_hbm,
    base_cos,
    base_sin,
    row_cos,
    row_sin,
    out_ref,
    tokens,
    dq,
    dl,
    dr,
    uq,
    ur,
    uk,
    uv,
    ow,
    kv,
    ql,
    qh,
    acc,
    best,
    att,
    pair_out,
    pair_in,
    kept,
    cross_out,
    cross_in,
    uvt,
    first_keys,
    first_values,
    cos_ref,
    sin_ref,
    load_sem,
    line_send,
    line_recv,
    kv_send,
    kv_recv,
    beside_send,
    beside_recv,
    q_send,
    q_recv,
    pair_send,
    pair_recv,
    cross_send,
    cross_recv,
):
    O = S // 2
    rows = tokens.shape[0]
    span = rows * T
    depth = tokens.shape[1]
    heads = qh.shape[0]
    rank = dl.shape[1]
    sp = lax.axis_index("sp")
    tp = lax.axis_index("tp")
    o, i = sp // 2, sp % 2
    g, c = tp // 2, tp % 2
    Y = int(O**0.5)
    z, y = o // Y, o % Y

    def dev(o_, i_, g_, c_):
        return {"sp": o_ * 2 + i_, "tp": g_ * 2 + c_}

    across = dev(o, i, 1 - g, c)
    beside = dev(o, 1 - i, g, c)
    mate = dev(o, i, g, 1 - c)

    step = depth // chunks
    loads = []

    def load(src, dst):
        copy = pltpu.make_async_copy(src, dst, load_sem.at[len(loads)])
        loads.append(copy)
        copy.start()
        return copy

    tok_load = load(tokens_hbm, tokens)
    dl_loads = [load(dl_hbm.at[pl.ds(k * step, step)], dl.at[pl.ds(k * step, step)]) for k in range(chunks)]
    dr_load = load(dr_hbm, dr)
    dq_loads = [load(dq_hbm.at[pl.ds(k * step, step)], dq.at[pl.ds(k * step, step)]) for k in range(chunks)]
    up_loads = [load(uq_hbm, uq), load(ur_hbm, ur), load(uk_hbm, uk), load(uv_hbm, uv)]
    ow_load = load(ow_hbm, ow)

    barrier = pltpu.get_barrier_semaphore()
    for step_ in (1, Y - 1):
        for node_ in (z * Y + (y + step_) % Y, (z + step_) % Y * Y + y):
            pl.semaphore_signal(barrier, inc=1, device_id={"sp": node_ * 2 + i, "tp": tp}, device_id_type=MESH)
    for n in range(1, T):
        pl.semaphore_signal(barrier, inc=1, device_id={"sp": sp, "tp": (tp + n) % T}, device_id_type=MESH)
    pl.semaphore_signal(barrier, inc=1, device_id=beside, device_id_type=MESH)

    def block_rows(b):
        return pl.ds(pl.multiple_of(b * rows, rows), rows)

    mine = block_rows(sp * T + tp)
    half = span // 2
    first_pos = jnp.where(i == 0, y, z)
    second_pos = jnp.where(i == 0, z, y)

    def node(da, db, i_):
        a_ = (jnp.where(i_ == 0, y, z) + da) % Y
        b_ = (jnp.where(i_ == 0, z, y) + db) % Y
        return jnp.where(i_ == 0, b_ * Y + a_, a_ * Y + b_)

    def send(part, target, send_sem, recv_sem):
        return pltpu.make_async_remote_copy(
            src_ref=part,
            dst_ref=part,
            send_sem=send_sem,
            recv_sem=recv_sem,
            device_id=target,
            device_id_type=MESH,
        )

    def near(t):
        return {"sp": o * 2 + i, "tp": t}

    def ring(da, db):
        return {"sp": node(da, db, i) * 2 + i, "tp": tp}

    def line_copy(n):
        return send(kv.at[mine], near((tp + n) % T), line_send.at[n], line_recv.at[tp])

    def line_wait(n):
        t = (tp + n) % T
        part = kv.at[block_rows(sp * T + t)]
        send(part, near(t), line_send.at[n], line_recv.at[t]).wait_recv()

    def half_part(s, h):
        return kv.at[pl.ds(pl.multiple_of(s * span + h * half, half), half)]

    def half_copy(s, h, target, index):
        return send(half_part(s, h), target, kv_send.at[index], kv_recv.at[s * 2 + h])

    def half_wait(s, h):
        half_copy(s, h, beside, 0).wait_recv()

    def beside_copy(s, index):
        part = kv.at[pl.ds(pl.multiple_of(s * span, span), span)]
        return send(part, beside, beside_send.at[index], beside_recv.at[s])

    def steps(k):
        da = db = 0
        for n, (p, q) in enumerate(EVENTS):
            da = jnp.where(k == n, p, da)
            db = jnp.where(k == n, q, db)
        return da, db

    def first_ring(act):
        for h in range(2):
            act(half_copy(sp, h, ring(1, 0), h))
            act(half_copy(sp, 1 - h, ring(Y - 1, 0), 2 + h))

    def second_ring(s, da, act):
        for h in range(2):
            act(half_copy(s, h, ring(0, 1), 4 + da * 4 + h))
            act(half_copy(s, 1 - h, ring(0, Y - 1), 4 + da * 4 + 2 + h))

    def relay(s, k, da, db):
        along = jnp.where(db == 0, da, db)
        way = jnp.where(along == 1, Y - 1, 1)
        h = jnp.where(along == 1, 1, 0)
        target = ring(jnp.where(db == 0, way, 0), jnp.where(db == 0, 0, way))
        return along, h, half_copy(s, h, target, 4 + 4 * Y + k)

    def forward(k):
        da, db = steps(k)
        s = node(da, db, i) * 2 + i
        along, h, copy = relay(s, k, da, db)
        half_wait(s, h)
        pl.when(along != 2)(copy.start)
        half_wait(s, 1 - h)
        pl.when(db == 0)(lambda: second_ring(s, da, start))
        beside_copy(s, k).start()

    def start(copy):
        copy.start()

    def sent(copy):
        copy.wait_send()

    start_cos, start_sin = base_cos[pl.ds(sp, 1), :], base_sin[pl.ds(sp, 1), :]
    sign = jnp.where(lax.broadcasted_iota(jnp.int32, (1, LANES), 1) % ROPE < ROPE // 2, -1.0, 1.0)
    cos_ref[...] = start_cos * row_cos[...] - start_sin * row_sin[...]
    sin_ref[...] = (start_sin * row_cos[...] + start_cos * row_sin[...]) * sign

    tok_load.wait()
    latent = jnp.zeros((rows, rank), F32)
    for k in range(chunks):
        dl_loads[k].wait()
        latent += dot(tokens[:, k * step : (k + 1) * step], dl[k * step : (k + 1) * step, :])
    dr_load.wait()
    turned = dot_nt(tokens[...], dr[...])
    turned = jnp.concatenate([turned, jnp.zeros((rows, LANES - ROPE), F32)], axis=1)
    own_rows = pl.ds(pl.multiple_of(tp * rows, rows), rows)
    kv[mine, :rank] = normed(latent, lg_ref[...]).astype(BF16)
    kv[mine, rank:] = turn(turned, cos_ref[own_rows, :], sin_ref[own_rows, :]).astype(BF16)

    pl.semaphore_wait(barrier, 4 + T - 1 + 1)
    for n in range(1, T):
        line_copy(n).start()

    query = jnp.zeros((rows, dq.shape[1]), F32)
    for k in range(chunks):
        dq_loads[k].wait()
        query += dot(tokens[:, k * step : (k + 1) * step], dq[k * step : (k + 1) * step, :])
    ql[own_rows, :] = normed(query, qg_ref[...]).astype(BF16)

    def q_copy(n):
        return send(ql.at[own_rows], near((tp + n) % T), q_send.at[n], q_recv.at[tp])

    def q_wait(n):
        t = (tp + n) % T
        send(ql.at[block_rows(t)], near(t), q_send.at[n], q_recv.at[t]).wait_recv()

    for n in range(1, T):
        q_copy(n).start()
    for n in range(1, T):
        line_wait(n)
    first_ring(start)
    second_ring(sp, 0, start)
    beside_copy(sp, 0).start()

    def kv_heads(s):
        part = pl.ds(pl.multiple_of(s * span, span), span)
        lat = kv[part, :rank]
        return dot(lat, uk[...]).astype(BF16), dot_nt(uvt[...], lat).astype(BF16)

    up_loads[2].wait()
    up_loads[3].wait()
    uvt[...] = uv[...].T
    first_keys[...], first_values[...] = kv_heads(sp)
    for n in range(1, T):
        q_wait(n)
    for copy in up_loads[:2]:
        copy.wait()
    scale = (NOPE + ROPE) ** (-0.5) * log2e
    plain = (dot(ql[...], uq[...]) * scale).astype(BF16)
    turning = dot(ql[...], ur[...]) * scale
    low = lax.broadcasted_iota(jnp.int32, (span, LANES), 1) < ROPE
    for pair in range(heads // 2):
        both = turn(turning[:, pair * LANES : (pair + 1) * LANES], cos_ref[...], sin_ref[...])
        qh[2 * pair, :, NOPE:] = jnp.where(low, both, 0.0).astype(BF16)
        qh[2 * pair + 1, :, NOPE:] = jnp.where(low, pltpu.roll(both, ROPE, 1), 0.0).astype(BF16)
    for h in range(heads):
        qh[h, :, :NOPE] = plain[:, h * NOPE : (h + 1) * NOPE]
        best[h] = jnp.full(best.shape[1:], masked_score, F32)
        acc[h] = jnp.zeros(acc.shape[1:], F32)

    def attend(s, masked=False):
        rot = kv[pl.ds(pl.multiple_of(s * span, span), span), rank:]
        keys, values = (first_keys[...], first_values[...]) if masked else kv_heads(s)
        ones = jnp.ones((acc.shape[1] - VDIM, span), BF16)
        if masked:
            k_pos = lax.broadcasted_iota(jnp.int32, (span, span), 0)
            q_pos = lax.broadcasted_iota(jnp.int32, (span, span), 1)
            allowed = k_pos <= q_pos

        def score(h):
            key = jnp.concatenate([keys[:, h * NOPE : (h + 1) * NOPE], rot], axis=1)
            return dot_nt(key, qh[h])

        ahead = score(0)
        for h in range(heads):
            scores = ahead
            if h + 1 < heads:
                ahead = score(h + 1)
            value = jnp.concatenate([values[h * VDIM : (h + 1) * VDIM], ones], axis=0)
            if masked:
                scores = jnp.where(allowed, scores, masked_score)
            old = best[h][:1]
            new = jnp.maximum(old, jnp.max(scores, axis=0, keepdims=True))
            weights = jnp.exp2(scores - new).astype(BF16)
            acc[h] = acc[h] * jnp.exp2(old - new) + dot(value, weights)
            best[h] = jnp.broadcast_to(new, best.shape[1:])

    def partner(k):
        da, db = steps(k)
        o_ = node(da, db, 1 - i)
        s = o_ * 2 + 1 - i
        beside_copy(s, k).wait_recv()
        pl.when(s < sp)(lambda: attend(s))

    def column(k, carry):
        pl.when(k + AHEAD < len(EVENTS))(lambda: forward(k + AHEAD))
        da, db = steps(k)
        o_ = node(da, db, i)
        pl.when(o_ < o)(lambda: attend(o_ * 2 + i))
        partner(k)
        return carry

    attend(sp, masked=True)
    for k in range(1, 1 + AHEAD):
        forward(k)
    partner(0)
    lax.fori_loop(1, len(EVENTS), column, 0)

    for h in range(heads):
        whole = acc[h]
        att[:, h * VDIM : (h + 1) * VDIM] = (whole[:VDIM] / whole[VDIM : VDIM + 1]).T.astype(BF16)

    ow_load.wait()
    width = ow.shape[1] // pieces
    lag = min(3, pieces)

    def pair_copy(phase, j):
        return pltpu.make_async_remote_copy(
            src_ref=pair_out.at[phase, j],
            dst_ref=pair_in.at[phase, j],
            send_sem=pair_send.at[phase * pieces + j],
            recv_sem=pair_recv.at[phase * pieces + j],
            device_id=mate,
            device_id_type=MESH,
        )

    def cross_copy(j):
        return pltpu.make_async_remote_copy(
            src_ref=cross_out.at[j],
            dst_ref=cross_in.at[j],
            send_sem=cross_send.at[j],
            recv_sem=cross_recv.at[j],
            device_id=across,
            device_id_type=MESH,
        )

    def project(phase, group, j):
        top = att[block_rows(group * 2 + 1 - c), :]
        low_part = att[block_rows(group * 2 + c), :]
        part = dot(jnp.concatenate([top, low_part], axis=0), ow[:, j * width : (j + 1) * width])
        pair_out[phase, j] = part[:rows].astype(BF16)
        kept[phase, j] = part[rows:]
        pair_copy(phase, j).start()

    def cross(j):
        pair_copy(0, j).wait_recv()
        cross_out[j] = (kept[0, j] + pair_in[0, j].astype(F32)).astype(BF16)
        cross_copy(j).start()

    for j in range(pieces):
        project(0, 1 - g, j)
        if j >= lag:
            cross(j - lag)
    for j in range(pieces - lag, pieces):
        cross(j)
    for j in range(pieces):
        project(1, g, j)
    for j in range(pieces):
        pair_copy(1, j).wait_recv()
        cross_copy(j).wait_recv()
        total = kept[1, j] + pair_in[1, j].astype(F32) + cross_in[j].astype(F32)
        out_ref[:, j * width : (j + 1) * width] = total

    def drain(k, carry):
        da, db = steps(k)
        s = node(da, db, i) * 2 + i
        along, h, copy = relay(s, k, da, db)
        pl.when(along != 2)(copy.wait_send)
        pl.when(db == 0)(lambda: second_ring(s, da, sent))
        beside_copy(s, k).wait_send()
        return carry

    lax.fori_loop(1, len(EVENTS), drain, 0)
    first_ring(sent)
    second_ring(sp, 0, sent)
    beside_copy(sp, 0).wait_send()
    for n in range(1, T):
        line_copy(n).wait_send()
        q_copy(n).wait_send()
    for j in range(pieces):
        pair_copy(0, j).wait_send()
        pair_copy(1, j).wait_send()
        cross_copy(j).wait_send()


def solution(mesh):
    S, T = mesh.shape["sp"], mesh.shape["tp"]
    assert S == 32 and T == 4

    def local(tokens, dq, dl, dr, qg, lg, uq, ur, uk, uv, ow):
        rows, depth = tokens.shape
        span = rows * T
        heads = uk.shape[1] // NOPE
        width = ow.shape[1]
        rank = dl.shape[1]
        chunks, pieces = 4, 8
        inverse = np.float32(rope_base) ** (-np.arange(0, ROPE, 2, dtype=np.float32) / np.float32(ROPE))
        inverse = np.tile(inverse.astype(np.float64), LANES // (ROPE // 2))
        starts = np.arange(S)[:, None] * span * inverse
        steps = np.arange(span)[:, None] * inverse
        tables = [jnp.asarray(f(a), F32) for a in (starts, steps) for f in (np.cos, np.sin)]
        O = S // 2
        hbm = pl.BlockSpec(memory_space=pl.ANY)
        vmem = pl.BlockSpec(memory_space=pltpu.VMEM)
        dma = lambda n: pltpu.SemaphoreType.DMA((n,))
        like = lambda a: pltpu.VMEM(a.shape, a.dtype)
        total = pl.pallas_call(
            functools.partial(kernel, S, T, chunks, pieces),
            out_shape=jax.ShapeDtypeStruct((rows, width), F32),
            in_specs=[hbm, hbm, hbm, hbm, vmem, vmem, hbm, hbm, hbm, hbm, hbm, vmem, vmem, vmem, vmem],
            out_specs=vmem,
            scratch_shapes=[
                like(tokens),
                like(dq),
                like(dl),
                pltpu.VMEM(dr.shape[::-1], dr.dtype),
                like(uq),
                like(ur),
                like(uk),
                like(uv),
                like(ow),
                pltpu.VMEM((S * span, rank + LANES), BF16),
                pltpu.VMEM((span, dq.shape[1]), BF16),
                pltpu.VMEM((heads, span, NOPE + LANES), BF16),
                pltpu.VMEM((heads, VDIM + 16, span), F32),
                pltpu.VMEM((heads, 8, span), F32),
                pltpu.VMEM((span, heads * VDIM), BF16),
                pltpu.VMEM((2, pieces, rows, width // pieces), BF16),
                pltpu.VMEM((2, pieces, rows, width // pieces), BF16),
                pltpu.VMEM((2, pieces, rows, width // pieces), F32),
                pltpu.VMEM((pieces, rows, width // pieces), BF16),
                pltpu.VMEM((pieces, rows, width // pieces), BF16),
                pltpu.VMEM(uv.shape[::-1], BF16),
                pltpu.VMEM((span, heads * NOPE), BF16),
                pltpu.VMEM((heads * VDIM, span), BF16),
                pltpu.VMEM((span, LANES), F32),
                pltpu.VMEM((span, LANES), F32),
                dma(2 * chunks + 7),
                dma(T),
                dma(T),
                dma(4 + 4 * 4 + O),
                dma(2 * S),
                dma(O),
                dma(S),
                dma(T),
                dma(T),
                dma(2 * pieces),
                dma(2 * pieces),
                dma(pieces),
                dma(pieces),
            ],
            compiler_params=pltpu.CompilerParams(
                collective_id=0, has_side_effects=True, vmem_limit_bytes=60 * 1024 * 1024
            ),
        )(
            tokens, dq, dl, dr.T, qg.reshape(1, -1), lg.reshape(1, -1),
            uq, ur, uk, uv, ow, *tables,
        )
        return total.astype(BF16)

    return jax.shard_map(
        local,
        mesh=mesh,
        in_specs=(
            P(("sp", "tp"), None),
            P(),
            P(),
            P(),
            P(),
            P(),
            P(None, "tp"),
            P(None, "tp"),
            P(None, "tp"),
            P(None, "tp"),
            P("tp", None),
        ),
        out_specs=P(("sp", "tp"), None),
        check_vma=False,
    )
```

```python
import functools

import jax
import jax.numpy as jnp
import numpy as np
from jax import lax
from jax.experimental import pallas as pl
from jax.experimental.pallas import tpu as pltpu
from jax.sharding import PartitionSpec as P

NOPE = 128
ROPE = 64
VDIM = 128
LANES = 128

rope_base = 500000.0
norm_eps = 1e-06
masked_score = -1e30
log2e = 1.4426950408889634

EVENTS = [
    (0, 0), (3, 0), (1, 0), (0, 3), (0, 1), (2, 0), (3, 3), (1, 3),
    (3, 1), (1, 1), (0, 2), (2, 3), (2, 1), (3, 2), (1, 2), (2, 2),
]
AHEAD = 2

MESH = pl.DeviceIdType.MESH
F32 = jnp.float32
BF16 = jnp.bfloat16


def dot(a, b):
    return jnp.dot(a, b, preferred_element_type=F32)


def dot_nt(a, b):
    return lax.dot_general(a, b, (((1,), (1,)), ((), ())), preferred_element_type=F32)


def turn(v, cosine, sine):
    lane = lax.broadcasted_iota(jnp.int32, v.shape, 1)
    other = jnp.where(lane % ROPE < ROPE // 2, pltpu.roll(v, LANES - ROPE // 2, 1), pltpu.roll(v, ROPE // 2, 1))
    return v * cosine + other * sine


def normed(v, gain):
    return v * lax.rsqrt(jnp.mean(v * v, axis=-1, keepdims=True) + norm_eps) * gain


def kernel(
    S,
    T,
    chunks,
    pieces,
    tokens_hbm,
    dq_hbm,
    dl_hbm,
    dr_hbm,
    qg_ref,
    lg_ref,
    uq_hbm,
    ur_hbm,
    uk_hbm,
    uv_hbm,
    ow_hbm,
    base_cos,
    base_sin,
    row_cos,
    row_sin,
    out_ref,
    tokens,
    dq,
    dl,
    dr,
    uq,
    ur,
    uk,
    uv,
    ow,
    kv,
    ql,
    qh,
    acc,
    best,
    att,
    side_out,
    side_in,
    kept,
    pass_out,
    pass_in,
    uvt,
    first_keys,
    first_values,
    cos_ref,
    sin_ref,
    load_sem,
    line_send,
    line_recv,
    kv_send,
    kv_recv,
    beside_send,
    beside_recv,
    q_send,
    q_recv,
    side_send,
    side_recv,
    pass_send,
    pass_recv,
):
    O = S // 2
    rows = tokens.shape[0]
    span = rows * T
    depth = tokens.shape[1]
    heads = qh.shape[0]
    rank = dl.shape[1]
    sp = lax.axis_index("sp")
    tp = lax.axis_index("tp")
    o, i = sp // 2, sp % 2
    Y = int(O**0.5)
    z, y = o // Y, o % Y
    beside = {"sp": o * 2 + 1 - i, "tp": tp}

    step = depth // chunks
    loads = []

    def load(src, dst):
        copy = pltpu.make_async_copy(src, dst, load_sem.at[len(loads)])
        loads.append(copy)
        copy.start()
        return copy

    tok_load = load(tokens_hbm, tokens)
    dl_loads = [load(dl_hbm.at[pl.ds(k * step, step)], dl.at[pl.ds(k * step, step)]) for k in range(chunks)]
    dr_load = load(dr_hbm, dr)
    dq_loads = [load(dq_hbm.at[pl.ds(k * step, step)], dq.at[pl.ds(k * step, step)]) for k in range(chunks)]
    up_loads = [load(uq_hbm, uq), load(ur_hbm, ur), load(uk_hbm, uk), load(uv_hbm, uv)]
    ow_load = load(ow_hbm, ow)

    barrier = pltpu.get_barrier_semaphore()
    for step_ in (1, Y - 1):
        for node_ in (z * Y + (y + step_) % Y, (z + step_) % Y * Y + y):
            pl.semaphore_signal(barrier, inc=1, device_id={"sp": node_ * 2 + i, "tp": tp}, device_id_type=MESH)
    for n in range(1, T):
        pl.semaphore_signal(barrier, inc=1, device_id={"sp": sp, "tp": (tp + n) % T}, device_id_type=MESH)
    pl.semaphore_signal(barrier, inc=1, device_id=beside, device_id_type=MESH)

    def block_rows(b):
        return pl.ds(pl.multiple_of(b * rows, rows), rows)

    mine = block_rows(sp * T + tp)
    half = span // 2
    first_pos = jnp.where(i == 0, y, z)
    second_pos = jnp.where(i == 0, z, y)

    def node(da, db, i_):
        a_ = (jnp.where(i_ == 0, y, z) + da) % Y
        b_ = (jnp.where(i_ == 0, z, y) + db) % Y
        return jnp.where(i_ == 0, b_ * Y + a_, a_ * Y + b_)

    def send(part, target, send_sem, recv_sem):
        return pltpu.make_async_remote_copy(
            src_ref=part,
            dst_ref=part,
            send_sem=send_sem,
            recv_sem=recv_sem,
            device_id=target,
            device_id_type=MESH,
        )

    def near(t):
        return {"sp": o * 2 + i, "tp": t}

    def ring(da, db):
        return {"sp": node(da, db, i) * 2 + i, "tp": tp}

    def line_copy(n):
        return send(kv.at[mine], near((tp + n) % T), line_send.at[n], line_recv.at[tp])

    def line_wait(n):
        t = (tp + n) % T
        part = kv.at[block_rows(sp * T + t)]
        send(part, near(t), line_send.at[n], line_recv.at[t]).wait_recv()

    def half_part(s, h):
        return kv.at[pl.ds(pl.multiple_of(s * span + h * half, half), half)]

    def half_copy(s, h, target, index):
        return send(half_part(s, h), target, kv_send.at[index], kv_recv.at[s * 2 + h])

    def half_wait(s, h):
        half_copy(s, h, beside, 0).wait_recv()

    def beside_copy(s, index):
        part = kv.at[pl.ds(pl.multiple_of(s * span, span), span)]
        return send(part, beside, beside_send.at[index], beside_recv.at[s])

    def steps(k):
        da = db = 0
        for n, (p, q) in enumerate(EVENTS):
            da = jnp.where(k == n, p, da)
            db = jnp.where(k == n, q, db)
        return da, db

    def first_ring(act):
        for h in range(2):
            act(half_copy(sp, h, ring(1, 0), h))
            act(half_copy(sp, 1 - h, ring(Y - 1, 0), 2 + h))

    def second_ring(s, da, act):
        for h in range(2):
            act(half_copy(s, h, ring(0, 1), 4 + da * 4 + h))
            act(half_copy(s, 1 - h, ring(0, Y - 1), 4 + da * 4 + 2 + h))

    def relay(s, k, da, db):
        along = jnp.where(db == 0, da, db)
        way = jnp.where(along == 1, Y - 1, 1)
        h = jnp.where(along == 1, 1, 0)
        target = ring(jnp.where(db == 0, way, 0), jnp.where(db == 0, 0, way))
        return along, h, half_copy(s, h, target, 4 + 4 * Y + k)

    def forward(k):
        da, db = steps(k)
        s = node(da, db, i) * 2 + i
        along, h, copy = relay(s, k, da, db)
        half_wait(s, h)
        pl.when(along != 2)(copy.start)
        half_wait(s, 1 - h)
        pl.when(db == 0)(lambda: second_ring(s, da, start))
        beside_copy(s, k).start()

    def start(copy):
        copy.start()

    def sent(copy):
        copy.wait_send()

    start_cos, start_sin = base_cos[pl.ds(sp, 1), :], base_sin[pl.ds(sp, 1), :]
    sign = jnp.where(lax.broadcasted_iota(jnp.int32, (1, LANES), 1) % ROPE < ROPE // 2, -1.0, 1.0)
    cos_ref[...] = start_cos * row_cos[...] - start_sin * row_sin[...]
    sin_ref[...] = (start_sin * row_cos[...] + start_cos * row_sin[...]) * sign

    tok_load.wait()
    latent = jnp.zeros((rows, rank), F32)
    for k in range(chunks):
        dl_loads[k].wait()
        latent += dot(tokens[:, k * step : (k + 1) * step], dl[k * step : (k + 1) * step, :])
    dr_load.wait()
    turned = dot_nt(tokens[...], dr[...])
    turned = jnp.concatenate([turned, jnp.zeros((rows, LANES - ROPE), F32)], axis=1)
    own_rows = pl.ds(pl.multiple_of(tp * rows, rows), rows)
    kv[mine, :rank] = normed(latent, lg_ref[...]).astype(BF16)
    kv[mine, rank:] = turn(turned, cos_ref[own_rows, :], sin_ref[own_rows, :]).astype(BF16)

    pl.semaphore_wait(barrier, 4 + T - 1 + 1)
    for n in range(1, T):
        line_copy(n).start()

    query = jnp.zeros((rows, dq.shape[1]), F32)
    for k in range(chunks):
        dq_loads[k].wait()
        query += dot(tokens[:, k * step : (k + 1) * step], dq[k * step : (k + 1) * step, :])
    ql[own_rows, :] = normed(query, qg_ref[...]).astype(BF16)

    def q_copy(n):
        return send(ql.at[own_rows], near((tp + n) % T), q_send.at[n], q_recv.at[tp])

    def q_wait(n):
        t = (tp + n) % T
        send(ql.at[block_rows(t)], near(t), q_send.at[n], q_recv.at[t]).wait_recv()

    for n in range(1, T):
        q_copy(n).start()
    for n in range(1, T):
        line_wait(n)
    first_ring(start)
    second_ring(sp, 0, start)
    beside_copy(sp, 0).start()

    def kv_heads(s):
        part = pl.ds(pl.multiple_of(s * span, span), span)
        lat = kv[part, :rank]
        return dot(lat, uk[...]).astype(BF16), dot_nt(uvt[...], lat).astype(BF16)

    up_loads[2].wait()
    up_loads[3].wait()
    uvt[...] = uv[...].T
    first_keys[...], first_values[...] = kv_heads(sp)
    for n in range(1, T):
        q_wait(n)
    for copy in up_loads[:2]:
        copy.wait()
    scale = (NOPE + ROPE) ** (-0.5) * log2e
    plain = (dot(ql[...], uq[...]) * scale).astype(BF16)
    turning = dot(ql[...], ur[...]) * scale
    low = lax.broadcasted_iota(jnp.int32, (span, LANES), 1) < ROPE
    for pair in range(heads // 2):
        both = turn(turning[:, pair * LANES : (pair + 1) * LANES], cos_ref[...], sin_ref[...])
        qh[2 * pair, :, NOPE:] = jnp.where(low, both, 0.0).astype(BF16)
        qh[2 * pair + 1, :, NOPE:] = jnp.where(low, pltpu.roll(both, ROPE, 1), 0.0).astype(BF16)
    for h in range(heads):
        qh[h, :, :NOPE] = plain[:, h * NOPE : (h + 1) * NOPE]
        best[h] = jnp.full(best.shape[1:], masked_score, F32)
        acc[h] = jnp.zeros(acc.shape[1:], F32)

    def attend(s, masked=False):
        rot = kv[pl.ds(pl.multiple_of(s * span, span), span), rank:]
        keys, values = (first_keys[...], first_values[...]) if masked else kv_heads(s)
        ones = jnp.ones((acc.shape[1] - VDIM, span), BF16)
        if masked:
            k_pos = lax.broadcasted_iota(jnp.int32, (span, span), 0)
            q_pos = lax.broadcasted_iota(jnp.int32, (span, span), 1)
            allowed = k_pos <= q_pos

        def score(h):
            key = jnp.concatenate([keys[:, h * NOPE : (h + 1) * NOPE], rot], axis=1)
            return dot_nt(key, qh[h])

        ahead = score(0)
        for h in range(heads):
            scores = ahead
            if h + 1 < heads:
                ahead = score(h + 1)
            value = jnp.concatenate([values[h * VDIM : (h + 1) * VDIM], ones], axis=0)
            if masked:
                scores = jnp.where(allowed, scores, masked_score)
            old = best[h][:1]
            new = jnp.maximum(old, jnp.max(scores, axis=0, keepdims=True))
            weights = jnp.exp2(scores - new).astype(BF16)
            acc[h] = acc[h] * jnp.exp2(old - new) + dot(value, weights)
            best[h] = jnp.broadcast_to(new, best.shape[1:])

    def partner(k):
        da, db = steps(k)
        o_ = node(da, db, 1 - i)
        s = o_ * 2 + 1 - i
        beside_copy(s, k).wait_recv()
        pl.when(s < sp)(lambda: attend(s))

    def column(k, carry):
        pl.when(k + AHEAD < len(EVENTS))(lambda: forward(k + AHEAD))
        da, db = steps(k)
        o_ = node(da, db, i)
        pl.when(o_ < o)(lambda: attend(o_ * 2 + i))
        partner(k)
        return carry

    attend(sp, masked=True)
    for k in range(1, 1 + AHEAD):
        forward(k)
    partner(0)
    lax.fori_loop(1, len(EVENTS), column, 0)

    for h in range(heads):
        whole = acc[h]
        att[:, h * VDIM : (h + 1) * VDIM] = (whole[:VDIM] / whole[VDIM : VDIM + 1]).T.astype(BF16)

    ow_load.wait()
    width = ow.shape[1] // pieces
    opposite, right, left = (tp + 2) % T, (tp + 1) % T, (tp + T - 1) % T

    def exchange(out, into, target, send_sem, recv_sem):
        return pltpu.make_async_remote_copy(
            src_ref=out,
            dst_ref=into,
            send_sem=send_sem,
            recv_sem=recv_sem,
            device_id=near(target),
            device_id_type=MESH,
        )

    def pass_copy(j):
        target = right if j < pieces // 2 else left
        return exchange(pass_out.at[j], pass_in.at[j], target, pass_send.at[j], pass_recv.at[j])

    def side_copy(side, j):
        n = side * pieces + j
        target = (right, left)[side]
        return exchange(side_out.at[side, j], side_in.at[side, j], target, side_send.at[n], side_recv.at[n])

    attended = jnp.concatenate([att[block_rows(t), :] for t in (opposite, right, left, tp)], axis=0)
    for n in range(pieces):
        j = n // 2 + n % 2 * (pieces // 2)
        late = 0 if j < pieces // 2 else 1
        part = dot(attended, ow[:, j * width : (j + 1) * width])
        pass_out[j] = part[:rows].astype(BF16)
        pass_copy(j).start()
        kept[0, j] = part[(1 + late) * rows : (2 + late) * rows]
        side_out[1 - late, j] = part[(2 - late) * rows : (3 - late) * rows].astype(BF16)
        kept[1, j] = part[3 * rows :]
    order = [n // 2 + n % 2 * (pieces // 2) for n in range(pieces)]
    for j in order:
        late = 0 if j < pieces // 2 else 1
        side_copy(1 - late, j).start()
    for j in order:
        late = 0 if j < pieces // 2 else 1
        pass_copy(j).wait_recv()
        side_out[late, j] = (kept[0, j] + pass_in[j].astype(F32)).astype(BF16)
        side_copy(late, j).start()
    for j in order:
        side_copy(0, j).wait_recv()
        side_copy(1, j).wait_recv()
        total = kept[1, j] + side_in[0, j].astype(F32) + side_in[1, j].astype(F32)
        out_ref[:, j * width : (j + 1) * width] = total.astype(BF16)

    def drain(k, carry):
        da, db = steps(k)
        s = node(da, db, i) * 2 + i
        along, h, copy = relay(s, k, da, db)
        pl.when(along != 2)(copy.wait_send)
        pl.when(db == 0)(lambda: second_ring(s, da, sent))
        beside_copy(s, k).wait_send()
        return carry

    lax.fori_loop(1, len(EVENTS), drain, 0)
    first_ring(sent)
    second_ring(sp, 0, sent)
    beside_copy(sp, 0).wait_send()
    for n in range(1, T):
        line_copy(n).wait_send()
        q_copy(n).wait_send()
    for j in range(pieces):
        pass_copy(j).wait_send()
        side_copy(0, j).wait_send()
        side_copy(1, j).wait_send()


def solution(mesh):
    S, T = mesh.shape["sp"], mesh.shape["tp"]
    assert S == 32 and T == 4

    def local(tokens, dq, dl, dr, qg, lg, uq, ur, uk, uv, ow):
        rows, depth = tokens.shape
        span = rows * T
        heads = uk.shape[1] // NOPE
        width = ow.shape[1]
        rank = dl.shape[1]
        chunks, pieces = 4, 8
        inverse = np.float32(rope_base) ** (-np.arange(0, ROPE, 2, dtype=np.float32) / np.float32(ROPE))
        inverse = np.tile(inverse.astype(np.float64), LANES // (ROPE // 2))
        starts = np.arange(S)[:, None] * span * inverse
        steps = np.arange(span)[:, None] * inverse
        tables = [jnp.asarray(f(a), F32) for a in (starts, steps) for f in (np.cos, np.sin)]
        O = S // 2
        hbm = pl.BlockSpec(memory_space=pl.ANY)
        vmem = pl.BlockSpec(memory_space=pltpu.VMEM)
        dma = lambda n: pltpu.SemaphoreType.DMA((n,))
        like = lambda a: pltpu.VMEM(a.shape, a.dtype)
        total = pl.pallas_call(
            functools.partial(kernel, S, T, chunks, pieces),
            out_shape=jax.ShapeDtypeStruct((rows, width), BF16),
            in_specs=[hbm, hbm, hbm, hbm, vmem, vmem, hbm, hbm, hbm, hbm, hbm, vmem, vmem, vmem, vmem],
            out_specs=vmem,
            scratch_shapes=[
                like(tokens),
                like(dq),
                like(dl),
                pltpu.VMEM(dr.shape[::-1], dr.dtype),
                like(uq),
                like(ur),
                like(uk),
                like(uv),
                like(ow),
                pltpu.VMEM((S * span, rank + LANES), BF16),
                pltpu.VMEM((span, dq.shape[1]), BF16),
                pltpu.VMEM((heads, span, NOPE + LANES), BF16),
                pltpu.VMEM((heads, VDIM + 16, span), F32),
                pltpu.VMEM((heads, 8, span), F32),
                pltpu.VMEM((span, heads * VDIM), BF16),
                pltpu.VMEM((2, pieces, rows, width // pieces), BF16),
                pltpu.VMEM((2, pieces, rows, width // pieces), BF16),
                pltpu.VMEM((2, pieces, rows, width // pieces), F32),
                pltpu.VMEM((pieces, rows, width // pieces), BF16),
                pltpu.VMEM((pieces, rows, width // pieces), BF16),
                pltpu.VMEM(uv.shape[::-1], BF16),
                pltpu.VMEM((span, heads * NOPE), BF16),
                pltpu.VMEM((heads * VDIM, span), BF16),
                pltpu.VMEM((span, LANES), F32),
                pltpu.VMEM((span, LANES), F32),
                dma(2 * chunks + 7),
                dma(T),
                dma(T),
                dma(4 + 4 * 4 + O),
                dma(2 * S),
                dma(O),
                dma(S),
                dma(T),
                dma(T),
                dma(2 * pieces),
                dma(2 * pieces),
                dma(pieces),
                dma(pieces),
            ],
            compiler_params=pltpu.CompilerParams(
                collective_id=0, has_side_effects=True, vmem_limit_bytes=60 * 1024 * 1024
            ),
        )(
            tokens, dq, dl, dr.T, qg.reshape(1, -1), lg.reshape(1, -1),
            uq, ur, uk, uv, ow, *tables,
        )
        return total

    return jax.shard_map(
        local,
        mesh=mesh,
        in_specs=(
            P(("sp", "tp"), None),
            P(),
            P(),
            P(),
            P(),
            P(),
            P(None, "tp"),
            P(None, "tp"),
            P(None, "tp"),
            P(None, "tp"),
            P("tp", None),
        ),
        out_specs=P(("sp", "tp"), None),
        check_vma=False,
    )
```

```python
import functools

import jax
import jax.numpy as jnp
import numpy as np
from jax import lax
from jax.experimental import pallas as pl
from jax.experimental.pallas import tpu as pltpu
from jax.sharding import PartitionSpec as P

NOPE = 128
ROPE = 64
VDIM = 128
LANES = 128

rope_base = 500000.0
norm_eps = 1e-06
masked_score = -1e30
log2e = 1.4426950408889634

EVENTS = [
    (0, 0), (3, 0), (1, 0), (0, 3), (0, 1), (2, 0), (3, 3), (1, 3),
    (3, 1), (1, 1), (0, 2), (2, 3), (2, 1), (3, 2), (1, 2), (2, 2),
]
AHEAD = 2

MESH = pl.DeviceIdType.MESH
F32 = jnp.float32
BF16 = jnp.bfloat16


def dot(a, b):
    return jnp.dot(a, b, preferred_element_type=F32)


def dot_nt(a, b):
    return lax.dot_general(a, b, (((1,), (1,)), ((), ())), preferred_element_type=F32)


def turn(v, cosine, sine):
    lane = lax.broadcasted_iota(jnp.int32, v.shape, 1)
    other = jnp.where(lane % ROPE < ROPE // 2, pltpu.roll(v, LANES - ROPE // 2, 1), pltpu.roll(v, ROPE // 2, 1))
    return v * cosine + other * sine


def normed(v, gain):
    return v * lax.rsqrt(jnp.mean(v * v, axis=-1, keepdims=True) + norm_eps) * gain


def kernel(
    S,
    T,
    chunks,
    pieces,
    tokens_hbm,
    dq_hbm,
    dl_hbm,
    dr_hbm,
    qg_ref,
    lg_ref,
    uq_hbm,
    ur_hbm,
    uk_hbm,
    uv_hbm,
    ow_hbm,
    base_cos,
    base_sin,
    row_cos,
    row_sin,
    out_hbm,
    tokens,
    dq,
    dl,
    dr,
    uq,
    ur,
    uk,
    uv,
    ow,
    kv,
    ql,
    qh,
    acc,
    best,
    att,
    side_out,
    side_in,
    kept,
    pass_out,
    pass_in,
    uvt,
    keys_a,
    values_a,
    keys_b,
    values_b,
    cos_ref,
    sin_ref,
    out,
    load_sem,
    out_sem,
    line_send,
    line_recv,
    kv_send,
    kv_recv,
    beside_send,
    beside_recv,
    q_send,
    q_recv,
    side_send,
    side_recv,
    pass_send,
    pass_recv,
):
    O = S // 2
    rows = tokens.shape[0]
    span = rows * T
    depth = tokens.shape[1]
    heads = qh.shape[0]
    rank = dl.shape[1]
    sp = lax.axis_index("sp")
    tp = lax.axis_index("tp")
    o, i = sp // 2, sp % 2
    Y = int(O**0.5)
    z, y = o // Y, o % Y
    beside = {"sp": o * 2 + 1 - i, "tp": tp}

    step = depth // chunks
    loads = []

    def load(src, dst):
        copy = pltpu.make_async_copy(src, dst, load_sem.at[len(loads)])
        loads.append(copy)
        copy.start()
        return copy

    tok_load = load(tokens_hbm, tokens)
    dl_loads = [load(dl_hbm.at[pl.ds(k * step, step)], dl.at[pl.ds(k * step, step)]) for k in range(chunks)]
    dr_load = load(dr_hbm, dr)
    dq_loads = [load(dq_hbm.at[pl.ds(k * step, step)], dq.at[pl.ds(k * step, step)]) for k in range(chunks)]
    up_loads = [load(uq_hbm, uq), load(ur_hbm, ur), load(uk_hbm, uk), load(uv_hbm, uv)]
    ow_load = load(ow_hbm, ow)

    barrier = pltpu.get_barrier_semaphore()
    for step_ in (1, Y - 1):
        for node_ in (z * Y + (y + step_) % Y, (z + step_) % Y * Y + y):
            pl.semaphore_signal(barrier, inc=1, device_id={"sp": node_ * 2 + i, "tp": tp}, device_id_type=MESH)
    for n in range(1, T):
        pl.semaphore_signal(barrier, inc=1, device_id={"sp": sp, "tp": (tp + n) % T}, device_id_type=MESH)
    pl.semaphore_signal(barrier, inc=1, device_id=beside, device_id_type=MESH)

    def block_rows(b):
        return pl.ds(pl.multiple_of(b * rows, rows), rows)

    mine = block_rows(sp * T + tp)
    half = span // 2
    first_pos = jnp.where(i == 0, y, z)
    second_pos = jnp.where(i == 0, z, y)

    def node(da, db, i_):
        a_ = (jnp.where(i_ == 0, y, z) + da) % Y
        b_ = (jnp.where(i_ == 0, z, y) + db) % Y
        return jnp.where(i_ == 0, b_ * Y + a_, a_ * Y + b_)

    def send(part, target, send_sem, recv_sem):
        return pltpu.make_async_remote_copy(
            src_ref=part,
            dst_ref=part,
            send_sem=send_sem,
            recv_sem=recv_sem,
            device_id=target,
            device_id_type=MESH,
        )

    def near(t):
        return {"sp": o * 2 + i, "tp": t}

    def ring(da, db):
        return {"sp": node(da, db, i) * 2 + i, "tp": tp}

    def line_part(ref, first, t, h):
        size = rows if h is None else rows // 2
        start_ = first + t * rows + (0 if h is None else h * size)
        return ref.at[pl.ds(pl.multiple_of(start_, size), size)]

    def around(ref, first, send_sem, recv_sem):
        ways = (1, T - 1)

        def own(n, act):
            part = line_part(ref, first, tp, None)
            act(send(part, near((tp + ways[n]) % T), send_sem.at[n], recv_sem.at[n]))

        def relay_on(n, act):
            part = line_part(ref, first, (tp + T - ways[n]) % T, n)
            act(send(part, near((tp + ways[n]) % T), send_sem.at[2 + n], recv_sem.at[2 + n]))

        def close_wait(n):
            t = (tp + T - ways[n]) % T
            send(line_part(ref, first, t, None), near(t), send_sem.at[n], recv_sem.at[n]).wait_recv()

        def far_wait(n):
            t = (tp + T // 2) % T
            send(line_part(ref, first, t, n), near(t), send_sem.at[2 + n], recv_sem.at[2 + n]).wait_recv()

        return own, relay_on, close_wait, far_wait

    kv_line = around(kv, sp * span, line_send, line_recv)
    q_line = around(ql, 0, q_send, q_recv)

    def half_part(s, h):
        return kv.at[pl.ds(pl.multiple_of(s * span + h * half, half), half)]

    def half_copy(s, h, target, index):
        return send(half_part(s, h), target, kv_send.at[index], kv_recv.at[s * 2 + h])

    def half_wait(s, h):
        half_copy(s, h, beside, 0).wait_recv()

    def beside_copy(s, index):
        part = kv.at[pl.ds(pl.multiple_of(s * span, span), span)]
        return send(part, beside, beside_send.at[index], beside_recv.at[s])

    def steps(k):
        da = db = 0
        for n, (p, q) in enumerate(EVENTS):
            da = jnp.where(k == n, p, da)
            db = jnp.where(k == n, q, db)
        return da, db

    def first_ring(act):
        for h in range(2):
            act(half_copy(sp, h, ring(1, 0), h))
            act(half_copy(sp, 1 - h, ring(Y - 1, 0), 2 + h))

    def second_ring(s, da, act):
        for h in range(2):
            act(half_copy(s, h, ring(0, 1), 4 + da * 4 + h))
            act(half_copy(s, 1 - h, ring(0, Y - 1), 4 + da * 4 + 2 + h))

    def relay(s, k, da, db):
        along = jnp.where(db == 0, da, db)
        way = jnp.where(along == 1, Y - 1, 1)
        h = jnp.where(along == 1, 1, 0)
        target = ring(jnp.where(db == 0, way, 0), jnp.where(db == 0, 0, way))
        return along, h, half_copy(s, h, target, 4 + 4 * Y + k)

    def forward(k):
        da, db = steps(k)
        s = node(da, db, i) * 2 + i
        along, h, copy = relay(s, k, da, db)
        half_wait(s, h)
        pl.when(along != 2)(copy.start)
        half_wait(s, 1 - h)
        pl.when(db == 0)(lambda: second_ring(s, da, start))
        beside_copy(s, k).start()

    def start(copy):
        copy.start()

    def sent(copy):
        copy.wait_send()

    start_cos, start_sin = base_cos[pl.ds(sp, 1), :], base_sin[pl.ds(sp, 1), :]
    sign = jnp.where(lax.broadcasted_iota(jnp.int32, (1, LANES), 1) % ROPE < ROPE // 2, -1.0, 1.0)
    cos_ref[...] = start_cos * row_cos[...] - start_sin * row_sin[...]
    sin_ref[...] = (start_sin * row_cos[...] + start_cos * row_sin[...]) * sign

    tok_load.wait()
    latent = jnp.zeros((rows, rank), F32)
    for k in range(chunks):
        dl_loads[k].wait()
        latent += dot(tokens[:, k * step : (k + 1) * step], dl[k * step : (k + 1) * step, :])
    dr_load.wait()
    turned = dot_nt(tokens[...], dr[...])
    turned = jnp.concatenate([turned, jnp.zeros((rows, LANES - ROPE), F32)], axis=1)
    own_rows = pl.ds(pl.multiple_of(tp * rows, rows), rows)
    kv[mine, :rank] = normed(latent, lg_ref[...]).astype(BF16)
    kv[mine, rank:] = turn(turned, cos_ref[own_rows, :], sin_ref[own_rows, :]).astype(BF16)

    pl.semaphore_wait(barrier, 4 + T - 1 + 1)
    for n in range(2):
        kv_line[0](n, start)

    query = jnp.zeros((rows, dq.shape[1]), F32)
    for k in range(chunks):
        dq_loads[k].wait()
        query += dot(tokens[:, k * step : (k + 1) * step], dq[k * step : (k + 1) * step, :])
    ql[own_rows, :] = normed(query, qg_ref[...]).astype(BF16)

    for n in range(2):
        kv_line[2](n)
        kv_line[1](n, start)
    for n in range(2):
        q_line[0](n, start)
    for n in range(2):
        kv_line[3](n)
    first_ring(start)
    second_ring(sp, 0, start)
    beside_copy(sp, 0).start()

    def key_rows(s):
        return pl.ds(pl.multiple_of(s * span, span), span)

    def project_keys(keys, n, s):
        keys[n * span : (n + 1) * span, :] = dot(kv[key_rows(s), :rank], uk[...]).astype(BF16)

    def project_values(values, n, s):
        values[:, n * span : (n + 1) * span] = dot_nt(uvt[...], kv[key_rows(s), :rank]).astype(BF16)

    up_loads[2].wait()
    up_loads[3].wait()
    uvt[...] = uv[...].T
    beside_copy(sp + 1 - 2 * i, 0).wait_recv()
    for n, s in enumerate((sp, sp + 1 - 2 * i)):
        project_keys(keys_a, n, s)
        project_values(values_a, n, s)
    for n in range(2):
        q_line[2](n)
        q_line[1](n, start)
    for n in range(2):
        q_line[3](n)
    for copy in up_loads[:2]:
        copy.wait()
    scale = (NOPE + ROPE) ** (-0.5) * log2e
    plain = (dot(ql[...], uq[...]) * scale).astype(BF16)
    turning = dot(ql[...], ur[...]) * scale
    low = lax.broadcasted_iota(jnp.int32, (span, LANES), 1) < ROPE
    for pair in range(heads // 2):
        both = turn(turning[:, pair * LANES : (pair + 1) * LANES], cos_ref[...], sin_ref[...])
        qh[2 * pair, :, NOPE:] = jnp.where(low, both, 0.0).astype(BF16)
        qh[2 * pair + 1, :, NOPE:] = jnp.where(low, pltpu.roll(both, ROPE, 1), 0.0).astype(BF16)
    for h in range(heads):
        qh[h, :, :NOPE] = plain[:, h * NOPE : (h + 1) * NOPE]
        best[h] = jnp.full(best.shape[1:], masked_score, F32)
        acc[h] = jnp.zeros(acc.shape[1:], F32)

    def pair_of(k):
        da, db = steps(k)
        own_, other_ = node(da, db, i) * 2 + i, node(da, db, 1 - i) * 2 + 1 - i
        return own_, other_

    def attend(keys, values, s, ahead_keys, ahead_values, ahead, masked=False):
        use = [t < sp for t in s]
        rot = jnp.concatenate([kv[key_rows(t), rank:] for t in s], axis=0)
        ones = jnp.ones((acc.shape[1] - VDIM, 2 * span), BF16)
        if masked:
            use[0] = sp >= 0
            k_pos = lax.broadcasted_iota(jnp.int32, (span, span), 0)
            q_pos = lax.broadcasted_iota(jnp.int32, (span, span), 1)
            allowed = k_pos <= q_pos
        penalty = [jnp.where(u, 0.0, -masked_score) for u in use]
        floor = [jnp.where(u, -masked_score, masked_score) for u in use]

        def score(h):
            key = jnp.concatenate([keys[:, h * NOPE : (h + 1) * NOPE], rot], axis=1)
            return dot_nt(key, qh[h])

        later = score(0)
        for h in range(heads):
            scores = later
            if h + 1 < heads:
                later = score(h + 1)
            if ahead is not None:
                if h % 2 == 0:
                    project_keys(ahead_keys, h // 2, ahead[h // 2])
                else:
                    project_values(ahead_values, h // 2, ahead[h // 2])
            value = jnp.concatenate([values[h * VDIM : (h + 1) * VDIM, :], ones], axis=0)
            parts = [scores[:span], scores[span:]]
            if masked:
                parts[0] = jnp.where(allowed, parts[0], masked_score)
            old = best[h][:1]
            new = old
            for part, limit in zip(parts, floor):
                new = jnp.maximum(new, jnp.minimum(jnp.max(part, axis=0, keepdims=True), limit))
            weights = [jnp.exp2(part - (new + extra)).astype(BF16) for part, extra in zip(parts, penalty)]
            acc[h] = acc[h] * jnp.exp2(old - new) + dot(value, jnp.concatenate(weights, axis=0))
            best[h] = jnp.broadcast_to(new, best.shape[1:])

    buffers = [(keys_a, values_a), (keys_b, values_b)]

    def arrive(k):
        pl.when(k + AHEAD < len(EVENTS))(lambda: forward(k + AHEAD))
        beside_copy(pair_of(k + 1)[1], 0).wait_recv()

    def step(k, slot):
        arrive(k)
        now, later = pair_of(k), pair_of(k + 1)
        any_ = (now[0] < sp) | (now[1] < sp) | (later[0] < sp) | (later[1] < sp)
        pl.when(any_)(lambda: attend(*buffers[slot], now, *buffers[1 - slot], later))

    for k in range(1, AHEAD):
        forward(k)
    arrive(0)
    attend(*buffers[0], (sp, sp + 1 - 2 * i), *buffers[1], pair_of(1), masked=True)

    def column(m, carry):
        step(2 * m + 1, 1)
        step(2 * m + 2, 0)
        return carry

    lax.fori_loop(0, len(EVENTS) // 2 - 1, column, 0)
    last = pair_of(len(EVENTS) - 1)
    pl.when((last[0] < sp) | (last[1] < sp))(lambda: attend(*buffers[1], last, None, None, None))

    for h in range(heads):
        whole = acc[h]
        att[:, h * VDIM : (h + 1) * VDIM] = (whole[:VDIM] / whole[VDIM : VDIM + 1]).T.astype(BF16)

    ow_load.wait()
    width = ow.shape[1] // pieces
    opposite, right, left = (tp + 2) % T, (tp + 1) % T, (tp + T - 1) % T

    def exchange(out, into, target, send_sem, recv_sem):
        return pltpu.make_async_remote_copy(
            src_ref=out,
            dst_ref=into,
            send_sem=send_sem,
            recv_sem=recv_sem,
            device_id=near(target),
            device_id_type=MESH,
        )

    def pass_copy(j):
        target = right if j < pieces // 2 else left
        return exchange(pass_out.at[j], pass_in.at[j], target, pass_send.at[j], pass_recv.at[j])

    def side_copy(side, j):
        n = side * pieces + j
        target = (right, left)[side]
        return exchange(side_out.at[side, j], side_in.at[side, j], target, side_send.at[n], side_recv.at[n])

    attended = jnp.concatenate([att[block_rows(t), :] for t in (opposite, right, left, tp)], axis=0)
    for n in range(pieces):
        j = n // 2 + n % 2 * (pieces // 2)
        late = 0 if j < pieces // 2 else 1
        part = dot(attended, ow[:, j * width : (j + 1) * width])
        pass_out[j] = part[:rows].astype(BF16)
        pass_copy(j).start()
        kept[0, j] = part[(1 + late) * rows : (2 + late) * rows]
        side_out[1 - late, j] = part[(2 - late) * rows : (3 - late) * rows].astype(BF16)
        kept[1, j] = part[3 * rows :]
    order = [n // 2 + n % 2 * (pieces // 2) for n in range(pieces)]
    for j in order:
        late = 0 if j < pieces // 2 else 1
        side_copy(1 - late, j).start()
    for j in order:
        late = 0 if j < pieces // 2 else 1
        pass_copy(j).wait_recv()
        side_out[late, j] = (kept[0, j] + pass_in[j].astype(F32)).astype(BF16)
        side_copy(late, j).start()

    def out_copy(j):
        part = pl.ds(j * width, width)
        return pltpu.make_async_copy(out.at[:, part], out_hbm.at[:, part], out_sem.at[j])

    for j in order:
        side_copy(0, j).wait_recv()
        side_copy(1, j).wait_recv()
        total = kept[1, j] + side_in[0, j].astype(F32) + side_in[1, j].astype(F32)
        out[:, j * width : (j + 1) * width] = total.astype(BF16)
        out_copy(j).start()

    def drain(k, carry):
        da, db = steps(k)
        s = node(da, db, i) * 2 + i
        along, h, copy = relay(s, k, da, db)
        pl.when(along != 2)(copy.wait_send)
        pl.when(db == 0)(lambda: second_ring(s, da, sent))
        beside_copy(s, k).wait_send()
        return carry

    lax.fori_loop(1, len(EVENTS), drain, 0)
    first_ring(sent)
    second_ring(sp, 0, sent)
    beside_copy(sp, 0).wait_send()
    for line in (kv_line, q_line):
        for n in range(2):
            line[0](n, sent)
            line[1](n, sent)
    for j in range(pieces):
        out_copy(j).wait()
        pass_copy(j).wait_send()
        side_copy(0, j).wait_send()
        side_copy(1, j).wait_send()


def solution(mesh):
    S, T = mesh.shape["sp"], mesh.shape["tp"]
    assert S == 32 and T == 4

    def local(tokens, dq, dl, dr, qg, lg, uq, ur, uk, uv, ow):
        rows, depth = tokens.shape
        span = rows * T
        heads = uk.shape[1] // NOPE
        width = ow.shape[1]
        rank = dl.shape[1]
        chunks, pieces = 4, 8
        inverse = np.float32(rope_base) ** (-np.arange(0, ROPE, 2, dtype=np.float32) / np.float32(ROPE))
        inverse = np.tile(inverse.astype(np.float64), LANES // (ROPE // 2))
        starts = np.arange(S)[:, None] * span * inverse
        steps = np.arange(span)[:, None] * inverse
        tables = [jnp.asarray(f(a), F32) for a in (starts, steps) for f in (np.cos, np.sin)]
        O = S // 2
        hbm = pl.BlockSpec(memory_space=pl.ANY)
        vmem = pl.BlockSpec(memory_space=pltpu.VMEM)
        dma = lambda n: pltpu.SemaphoreType.DMA((n,))
        like = lambda a: pltpu.VMEM(a.shape, a.dtype)
        total = pl.pallas_call(
            functools.partial(kernel, S, T, chunks, pieces),
            out_shape=jax.ShapeDtypeStruct((rows, width), BF16),
            in_specs=[hbm, hbm, hbm, hbm, vmem, vmem, hbm, hbm, hbm, hbm, hbm, vmem, vmem, vmem, vmem],
            out_specs=hbm,
            scratch_shapes=[
                like(tokens),
                like(dq),
                like(dl),
                pltpu.VMEM(dr.shape[::-1], dr.dtype),
                like(uq),
                like(ur),
                like(uk),
                like(uv),
                like(ow),
                pltpu.VMEM((S * span, rank + LANES), BF16),
                pltpu.VMEM((span, dq.shape[1]), BF16),
                pltpu.VMEM((heads, span, NOPE + LANES), BF16),
                pltpu.VMEM((heads, VDIM + 16, span), F32),
                pltpu.VMEM((heads, 8, span), F32),
                pltpu.VMEM((span, heads * VDIM), BF16),
                pltpu.VMEM((2, pieces, rows, width // pieces), BF16),
                pltpu.VMEM((2, pieces, rows, width // pieces), BF16),
                pltpu.VMEM((2, pieces, rows, width // pieces), F32),
                pltpu.VMEM((pieces, rows, width // pieces), BF16),
                pltpu.VMEM((pieces, rows, width // pieces), BF16),
                pltpu.VMEM(uv.shape[::-1], BF16),
                pltpu.VMEM((2 * span, heads * NOPE), BF16),
                pltpu.VMEM((heads * VDIM, 2 * span), BF16),
                pltpu.VMEM((2 * span, heads * NOPE), BF16),
                pltpu.VMEM((heads * VDIM, 2 * span), BF16),
                pltpu.VMEM((span, LANES), F32),
                pltpu.VMEM((span, LANES), F32),
                pltpu.VMEM((rows, width), BF16),
                dma(2 * chunks + 7),
                dma(pieces),
                dma(T),
                dma(T),
                dma(4 + 4 * 4 + O),
                dma(2 * S),
                dma(O),
                dma(S),
                dma(T),
                dma(T),
                dma(2 * pieces),
                dma(2 * pieces),
                dma(pieces),
                dma(pieces),
            ],
            compiler_params=pltpu.CompilerParams(
                collective_id=0, has_side_effects=True, vmem_limit_bytes=60 * 1024 * 1024
            ),
        )(
            tokens, dq, dl, dr.T, qg.reshape(1, -1), lg.reshape(1, -1),
            uq, ur, uk, uv, ow, *tables,
        )
        return total

    return jax.shard_map(
        local,
        mesh=mesh,
        in_specs=(
            P(("sp", "tp"), None),
            P(),
            P(),
            P(),
            P(),
            P(),
            P(None, "tp"),
            P(None, "tp"),
            P(None, "tp"),
            P(None, "tp"),
            P("tp", None),
        ),
        out_specs=P(("sp", "tp"), None),
        check_vma=False,
    )
```

```python
import functools

import jax
import jax.numpy as jnp
import numpy as np
from jax import lax
from jax.experimental import pallas as pl
from jax.experimental.pallas import tpu as pltpu
from jax.sharding import PartitionSpec as P

NOPE = 128
ROPE = 64
VDIM = 128
LANES = 128

rope_base = 500000.0
norm_eps = 1e-06
masked_score = -1e30
log2e = 1.4426950408889634

EVENTS = [
    (0, 0), (3, 0), (1, 0), (0, 3), (0, 1), (3, 3), (1, 3), (3, 1),
    (1, 1), (2, 0), (0, 2), (2, 3), (2, 1), (3, 2), (1, 2), (2, 2),
]
FAR = 9
NEXT = (11, 12)
PASS = {3: (11,), 4: (12,), 7: (15,)}
START = {3: (15,)}
SENT = 60
LEAD = 4
SENT_HALVES = 30

MESH = pl.DeviceIdType.MESH
F32 = jnp.float32
BF16 = jnp.bfloat16


def dot(a, b):
    return jnp.dot(a, b, preferred_element_type=F32)


def dot_nt(a, b):
    return lax.dot_general(a, b, (((1,), (1,)), ((), ())), preferred_element_type=F32)


def turn(v, cosine, sine):
    lane = lax.broadcasted_iota(jnp.int32, v.shape, 1)
    other = jnp.where(lane % ROPE < ROPE // 2, pltpu.roll(v, LANES - ROPE // 2, 1), pltpu.roll(v, ROPE // 2, 1))
    return v * cosine + other * sine


def normed(v, gain):
    return v * lax.rsqrt(jnp.mean(v * v, axis=-1, keepdims=True) + norm_eps) * gain


def kernel(
    S,
    T,
    chunks,
    pieces,
    tokens_hbm,
    dq_hbm,
    dl_hbm,
    dr_hbm,
    qg_hbm,
    lg_hbm,
    uq_hbm,
    ur_hbm,
    uk_hbm,
    uv_hbm,
    ow_hbm,
    base_hbm,
    turn_hbm,
    out_hbm,
    tokens,
    dq,
    dl,
    dr,
    uq,
    ur,
    uk,
    uv,
    ow,
    kv,
    ql,
    qh,
    acc,
    best,
    att,
    side_out,
    side_in,
    kept,
    pass_out,
    pass_in,
    uvt,
    keys_a,
    values_a,
    keys_b,
    values_b,
    keys_in,
    values_in,
    scores_a,
    scores_b,
    best_a,
    best_b,
    cos_ref,
    sin_ref,
    out,
    qg_ref,
    lg_ref,
    base,
    turns,
    load_sem,
    out_sem,
    line_send,
    line_recv,
    kv_send,
    kv_recv,
    share_send,
    share_recv,
    q_send,
    q_recv,
    side_send,
    side_recv,
    pass_send,
    pass_recv,
):
    O = S // 2
    rows = tokens.shape[0]
    span = rows * T
    depth = tokens.shape[1]
    heads = qh.shape[0]
    rank = dl.shape[1]
    sp = lax.axis_index("sp")
    tp = lax.axis_index("tp")
    o, i = sp // 2, sp % 2
    Y = int(O**0.5)
    z, y = o // Y, o % Y
    beside = {"sp": o * 2 + 1 - i, "tp": tp}

    step = depth // chunks
    loads = []

    def load(src, dst):
        copy = pltpu.make_async_copy(src, dst, load_sem.at[len(loads)])
        loads.append(copy)
        copy.start()
        return copy

    tok_load = load(tokens_hbm, tokens)
    small_loads = [load(lg_hbm, lg_ref), load(base_hbm, base), load(turn_hbm, turns), load(qg_hbm, qg_ref)]
    dl_loads = [load(dl_hbm.at[pl.ds(k * step, step)], dl.at[pl.ds(k * step, step)]) for k in range(chunks)]
    dr_load = load(dr_hbm, dr)
    dq_loads = [load(dq_hbm.at[pl.ds(k * step, step)], dq.at[pl.ds(k * step, step)]) for k in range(chunks)]
    barrier = pltpu.get_barrier_semaphore()
    for step_ in (1, Y - 1):
        for node_ in (z * Y + (y + step_) % Y, (z + step_) % Y * Y + y):
            pl.semaphore_signal(barrier, inc=1, device_id={"sp": node_ * 2 + i, "tp": tp}, device_id_type=MESH)
    for n in range(1, T):
        pl.semaphore_signal(barrier, inc=1, device_id={"sp": sp, "tp": (tp + n) % T}, device_id_type=MESH)
    pl.semaphore_signal(barrier, inc=1, device_id=beside, device_id_type=MESH)

    def block_rows(b):
        return pl.ds(pl.multiple_of(b * rows, rows), rows)

    mine = block_rows(o * T + tp)
    first_pos = jnp.where(i == 0, y, z)
    second_pos = jnp.where(i == 0, z, y)

    def node(da, db, i_):
        a_ = (jnp.where(i_ == 0, y, z) + da) % Y
        b_ = (jnp.where(i_ == 0, z, y) + db) % Y
        return jnp.where(i_ == 0, b_ * Y + a_, a_ * Y + b_)

    def send(part, target, send_sem, recv_sem):
        return pltpu.make_async_remote_copy(
            src_ref=part,
            dst_ref=part,
            send_sem=send_sem,
            recv_sem=recv_sem,
            device_id=target,
            device_id_type=MESH,
        )

    def near(t):
        return {"sp": o * 2 + i, "tp": t}

    def ring(da, db):
        return {"sp": node(da, db, i) * 2 + i, "tp": tp}

    def line_part(ref, first, t, h):
        size = rows if h is None else rows // 2
        start_ = first + t * rows + (0 if h is None else h * size)
        return ref.at[pl.ds(pl.multiple_of(start_, size), size)]

    def around(ref, first, send_sem, recv_sem):
        ways = (1, T - 1)

        def own(n):
            part = line_part(ref, first, tp, None)
            send(part, near((tp + ways[n]) % T), send_sem.at[0], recv_sem.at[n]).start()

        def relay_on(n):
            part = line_part(ref, first, (tp + T - ways[n]) % T, n)
            send(part, near((tp + ways[n]) % T), send_sem.at[0], recv_sem.at[2 + n]).start()

        def close_wait(n):
            t = (tp + T - ways[n]) % T
            send(line_part(ref, first, t, None), near(t), send_sem.at[0], recv_sem.at[n]).wait_recv()

        def far_wait(n):
            t = (tp + T // 2) % T
            send(line_part(ref, first, t, n), near(t), send_sem.at[0], recv_sem.at[2 + n]).wait_recv()

        return own, relay_on, close_wait, far_wait

    kv_line = around(kv, o * span, line_send, line_recv)
    q_line = around(ql, 0, q_send, q_recv)

    def sub_copy(n, t, target):
        part = kv.at[block_rows(n * T + t)]
        return send(part, target, kv_send.at[0], kv_recv.at[n * T + t])

    def sub_wait(n, t):
        sub_copy(n, t, beside).wait_recv()

    def steps(k):
        da = db = 0
        for n, (p, q) in enumerate(EVENTS):
            da = jnp.where(k == n, p, da)
            db = jnp.where(k == n, q, db)
        return da, db

    def beyond(j):
        return (tp + j) % T

    def first_ring(t):
        for way in (1, Y - 1):
            sub_copy(o, t, ring(way, 0)).start()

    def second_ring(n, t):
        for way in (1, Y - 1):
            sub_copy(n, t, ring(0, way)).start()

    def place(k):
        da, db = steps(k)
        return da, db, node(da, db, i)

    def early(k):
        da, db, n = place(k)
        sub_wait(n, tp)
        second_ring(n, tp)
        pl.when((i == 0) == (da == Y - 1))(sub_copy(n, tp, ring((Y - da) % Y, 0)).start)

    def rest(k):
        n = place(k)[2]
        for j in (1, 3, 2):
            sub_wait(n, beyond(j))
            second_ring(n, beyond(j))

    def whole(k):
        da, db, n = place(k)
        for j in (0, 1, 3, 2):
            sub_wait(n, beyond(j))
            way = Y - 1 if j in (3, 2) else 1
            pl.when(db == Y - way)(sub_copy(n, beyond(j), ring(0, way)).start)

    def cross_start(k):
        da, db, n = place(k)
        sub_wait(n, tp)
        pl.when(db == 0)(lambda: second_ring(n, tp))
        pl.when(db == jnp.where(i == 0, Y - 1, 1))(sub_copy(n, tp, ring(0, (Y - db) % Y)).start)
        for way in (1, T - 1):
            sub_copy(n, tp, near(beyond(way))).start()

    def cross_pass(k):
        da, db, n = place(k)
        for way in (1, T - 1):
            sub_wait(n, beyond(T - way))
        way = jnp.where((db + i) % 2 == 0, 1, T - 1)
        sub_copy(n, (tp + T - way) % T, near((tp + way) % T)).start()

    def cross_end(k):
        sub_wait(place(k)[2], beyond(2))

    tok_load.wait()
    latent = jnp.zeros((rows, rank), F32)
    for k in range(chunks):
        dl_loads[k].wait()
        latent += dot(tokens[:, k * step : (k + 1) * step], dl[k * step : (k + 1) * step, :])
    dr_load.wait()
    for copy in small_loads:
        copy.wait()
    start_cos, start_sin = base[0, pl.ds(sp, 1), :], base[1, pl.ds(sp, 1), :]
    sign = jnp.where(lax.broadcasted_iota(jnp.int32, (1, LANES), 1) % ROPE < ROPE // 2, -1.0, 1.0)
    cos_ref[...] = start_cos * turns[0] - start_sin * turns[1]
    sin_ref[...] = (start_sin * turns[0] + start_cos * turns[1]) * sign
    turned = dot_nt(tokens[...], dr[...])
    turned = jnp.concatenate([turned, jnp.zeros((rows, LANES - ROPE), F32)], axis=1)
    own_rows = pl.ds(pl.multiple_of(tp * rows, rows), rows)
    kv[mine, :rank] = normed(latent, lg_ref[...]).astype(BF16)
    kv[mine, rank:] = turn(turned, cos_ref[own_rows, :], sin_ref[own_rows, :]).astype(BF16)

    up_loads = [load(uq_hbm, uq), load(ur_hbm, ur), load(uk_hbm, uk), load(uv_hbm, uv)]
    ow_load = load(ow_hbm, ow)
    pl.semaphore_wait(barrier, 4 + T - 1 + 1)
    for n in range(2):
        kv_line[0](n)
    first_ring(tp)
    second_ring(o, tp)

    query = jnp.zeros((rows, dq.shape[1]), F32)
    for k in range(chunks):
        dq_loads[k].wait()
        query += dot(tokens[:, k * step : (k + 1) * step], dq[k * step : (k + 1) * step, :])
    ql[own_rows, :] = normed(query, qg_ref[...]).astype(BF16)

    early(1)
    early(2)
    for n in range(2):
        kv_line[2](n)
        kv_line[1](n)
    for n in range(2):
        q_line[0](n)
    for j in (1, 3):
        first_ring(beyond(j))
        second_ring(o, beyond(j))
    for n in range(2):
        kv_line[3](n)
    first_ring(beyond(2))
    second_ring(o, beyond(2))

    def spot(k):
        n = node(*steps(k), i)
        return pl.ds(pl.multiple_of(n * span, span), span)

    def project_keys(k, parity):
        keys = own_keys[parity]
        keys[k // 2, :, : heads * NOPE] = dot(kv[spot(k), :rank], uk[...]).astype(BF16)
        keys[k // 2, :, heads * NOPE :] = kv[spot(k), rank:]

    def project_values(k, parity):
        own_values[parity][k // 2] = dot_nt(uvt[...], kv[spot(k), :rank]).astype(BF16)

    own_keys, own_values = (keys_a, keys_b), (values_a, values_b)
    kept_scores, kept_best = (scores_a, scores_b), (best_a, best_b)

    def share(n, k, parity):
        own, into = ((own_keys, keys_in), (own_values, values_in))[n]
        return pltpu.make_async_remote_copy(
            src_ref=own[parity].at[k // 2],
            dst_ref=into.at[k],
            send_sem=share_send.at[n],
            recv_sem=share_recv.at[n * O + k],
            device_id=beside,
            device_id_type=MESH,
        )

    def prepare_keys(k):
        project_keys(k, k % 2)
        share(0, k, k % 2).start()

    def prepare_values(k):
        project_values(k, k % 2)
        share(1, k, k % 2).start()

    up_loads[2].wait()
    up_loads[3].wait()
    uvt[...] = uv[...].T
    prepare_keys(0)
    prepare_values(0)
    cross_start(FAR)
    for n in range(2):
        q_line[2](n)
        q_line[1](n)
    for k in range(1, 3):
        rest(k)
        prepare_keys(k)
        prepare_values(k)
    cross_pass(FAR)
    for n in range(2):
        q_line[3](n)
    for copy in up_loads[:2]:
        copy.wait()
    scale = (NOPE + ROPE) ** (-0.5) * log2e
    plain = (dot(ql[...], uq[...]) * scale).astype(BF16)
    turning = dot(ql[...], ur[...]) * scale
    low = lax.broadcasted_iota(jnp.int32, (span, LANES), 1) < ROPE
    for pair in range(heads // 2):
        both = turn(turning[:, pair * LANES : (pair + 1) * LANES], cos_ref[...], sin_ref[...])
        qh[2 * pair, :, NOPE:] = jnp.where(low, both, 0.0).astype(BF16)
        qh[2 * pair + 1, :, NOPE:] = jnp.where(low, pltpu.roll(both, ROPE, 1), 0.0).astype(BF16)
    for h in range(heads):
        qh[h, :, :NOPE] = plain[:, h * NOPE : (h + 1) * NOPE]
        best[h] = jnp.full(best.shape[1:], masked_score, F32)
        acc[h] = jnp.zeros(acc.shape[1:], F32)

    def used(k):
        first = k == 0
        mine_, other_ = node(*steps(k), i), node(*steps(k), 1 - i)
        return (mine_ < o) | first, (other_ < o) | (first & (i == 1))

    def score(k, parity, h, masked=False):
        keys = own_keys[parity]
        part = slice(h * NOPE, (h + 1) * NOPE)
        rot = jnp.concatenate([keys[k // 2, :, heads * NOPE :], keys_in[k, :, heads * NOPE :]], axis=0)
        key = jnp.concatenate([keys[k // 2, :, part], keys_in[k, :, part]], axis=0)
        scores = dot_nt(jnp.concatenate([key, rot], axis=1), qh[h])
        pieces_ = [scores[:span], scores[span:]]
        if masked:
            k_pos = lax.broadcasted_iota(jnp.int32, (span, span), 0)
            q_pos = lax.broadcasted_iota(jnp.int32, (span, span), 1)
            pieces_[0] = jnp.where(k_pos <= q_pos, pieces_[0], masked_score)
        top = None
        for n, (piece, use) in enumerate(zip(pieces_, used(k))):
            kept_scores[parity][h, n * span : (n + 1) * span, :] = piece
            limit = jnp.where(use, -masked_score, masked_score)
            new = jnp.minimum(jnp.max(piece, axis=0, keepdims=True), limit)
            top = new if top is None else jnp.maximum(top, new)
        kept_best[parity][h] = jnp.broadcast_to(top, best.shape[1:])

    ones = jnp.ones((acc.shape[1] - VDIM, 2 * span), BF16)

    def weigh(k, parity, h):
        part = slice(h * VDIM, (h + 1) * VDIM)
        value = jnp.concatenate([own_values[parity][k // 2, part, :], values_in[k, part, :]], axis=1)
        value = jnp.concatenate([value, ones], axis=0)
        old = best[h][:1]
        new = jnp.maximum(old, kept_best[parity][h][:1])
        weights = []
        for n, use in enumerate(used(k)):
            shift = new + jnp.where(use, 0.0, -masked_score)
            weights.append(jnp.exp2(kept_scores[parity][h, n * span : (n + 1) * span, :] - shift).astype(BF16))
        acc[h] = acc[h] * jnp.exp2(old - new) + dot(value, jnp.concatenate(weights, axis=0))
        best[h] = jnp.broadcast_to(new, best.shape[1:])

    count = len(EVENTS)

    def step(k, parity, scoring=True, keying=True, valuing=True):
        if keying:
            far = steps(k + LEAD)[0] == Y // 2
            pl.when(far)(lambda: cross_end(k + LEAD))
            pl.when(~far)(lambda: whole(k + LEAD))
            for table, act in ((PASS, cross_pass), (START, cross_start)):
                for n, events in table.items():
                    if n % 2 == parity:
                        pl.when(k == n)(lambda events=events, act=act: [act(e) for e in events][0])
        if scoring:
            share(0, k + 1, 1 - parity).wait_recv()
        share(1, k, parity).wait_recv()
        needed = used(k)[0] | used(k)[1]
        if scoring:
            needed = needed | used(k + 1)[0] | used(k + 1)[1]

        @pl.when(needed)
        def _():
            for h in range(heads):
                if scoring:
                    score(k + 1, 1 - parity, h)
                if keying and h == 0:
                    project_keys(k + LEAD, parity)
                if valuing and h == 2:
                    project_values(k + LEAD - 1, 1 - parity)
                weigh(k, parity, h)

        @pl.when(~needed)
        def _():
            if keying:
                project_keys(k + LEAD, parity)
            if valuing:
                project_values(k + LEAD - 1, 1 - parity)

        if keying:
            share(0, k + LEAD, parity).start()
        if valuing:
            share(1, k + LEAD - 1, 1 - parity).start()

    share(0, 0, 0).wait_recv()
    for h in range(heads):
        score(0, 0, h, masked=True)
    for k in NEXT:
        cross_start(k)
    whole(3)
    prepare_keys(3)

    def column(m, carry):
        step(2 * m, 0)
        step(2 * m + 1, 1)
        return carry

    lax.fori_loop(0, (count - LEAD) // 2, column, 0)
    for k in range(count - LEAD, count):
        step(k, k % 2, scoring=k + 1 < count, keying=k + LEAD < count, valuing=k + LEAD - 1 < count)

    for h in range(heads):
        whole = acc[h]
        att[:, h * VDIM : (h + 1) * VDIM] = (whole[:VDIM] / whole[VDIM : VDIM + 1]).T.astype(BF16)

    ow_load.wait()
    width = ow.shape[1] // pieces
    opposite, right, left = (tp + 2) % T, (tp + 1) % T, (tp + T - 1) % T

    def exchange(out, into, target, send_sem, recv_sem):
        return pltpu.make_async_remote_copy(
            src_ref=out,
            dst_ref=into,
            send_sem=send_sem,
            recv_sem=recv_sem,
            device_id=near(target),
            device_id_type=MESH,
        )

    def pass_copy(j):
        target = right if j < pieces // 2 else left
        return exchange(pass_out.at[j], pass_in.at[j], target, pass_send.at[0], pass_recv.at[j])

    def side_copy(side, j):
        n = side * pieces + j
        target = (right, left)[side]
        return exchange(side_out.at[side, j], side_in.at[side, j], target, side_send.at[0], side_recv.at[n])

    attended = jnp.concatenate([att[block_rows(t), :] for t in (opposite, right, left, tp)], axis=0)
    for n in range(pieces):
        j = n // 2 + n % 2 * (pieces // 2)
        late = 0 if j < pieces // 2 else 1
        part = dot(attended, ow[:, j * width : (j + 1) * width])
        pass_out[j] = part[:rows].astype(BF16)
        pass_copy(j).start()
        kept[0, j] = part[(1 + late) * rows : (2 + late) * rows]
        side_out[1 - late, j] = part[(2 - late) * rows : (3 - late) * rows].astype(BF16)
        kept[1, j] = part[3 * rows :]
    order = [n // 2 + n % 2 * (pieces // 2) for n in range(pieces)]
    for j in order:
        late = 0 if j < pieces // 2 else 1
        side_copy(1 - late, j).start()
    for j in order:
        late = 0 if j < pieces // 2 else 1
        pass_copy(j).wait_recv()
        side_out[late, j] = (kept[0, j] + pass_in[j].astype(F32)).astype(BF16)
        side_copy(late, j).start()

    def out_copy(j):
        part = pl.ds(j * width, width)
        return pltpu.make_async_copy(out.at[:, part], out_hbm.at[:, part], out_sem.at[0])

    for j in order:
        side_copy(0, j).wait_recv()
        side_copy(1, j).wait_recv()
        total = kept[1, j] + side_in[0, j].astype(F32) + side_in[1, j].astype(F32)
        out[:, j * width : (j + 1) * width] = total.astype(BF16)
        out_copy(j).start()

    def all_sent(ref, send_sem):
        send(ref, beside, send_sem.at[0], send_sem.at[0]).wait_send()

    all_sent(kv.at[pl.ds(0, SENT * rows)], kv_send)
    for n, refs in enumerate((own_keys, own_values)):
        for ref in refs:
            send(ref, beside, share_send.at[n], share_send.at[n]).wait_send()
    all_sent(kv.at[pl.ds(0, 3 * rows)], line_send)
    all_sent(ql.at[pl.ds(0, 3 * rows)], q_send)
    all_sent(side_out, side_send)
    all_sent(pass_out, pass_send)
    pltpu.make_async_copy(out, out_hbm, out_sem.at[0]).wait()


def solution(mesh):
    S, T = mesh.shape["sp"], mesh.shape["tp"]
    assert S == 32 and T == 4

    def local(tokens, dq, dl, dr, qg, lg, uq, ur, uk, uv, ow):
        rows, depth = tokens.shape
        span = rows * T
        heads = uk.shape[1] // NOPE
        width = ow.shape[1]
        rank = dl.shape[1]
        chunks, pieces = 4, 8
        inverse = np.float32(rope_base) ** (-np.arange(0, ROPE, 2, dtype=np.float32) / np.float32(ROPE))
        inverse = np.tile(inverse.astype(np.float64), LANES // (ROPE // 2))
        starts = np.arange(S)[:, None] * span * inverse
        steps = np.arange(span)[:, None] * inverse
        tables = [jnp.asarray(np.stack([np.cos(a), np.sin(a)]), F32) for a in (starts, steps)]
        O = S // 2
        hbm = pl.BlockSpec(memory_space=pl.ANY)
        dma = lambda n: pltpu.SemaphoreType.DMA((n,))
        like = lambda a: pltpu.VMEM(a.shape, a.dtype)
        total = pl.pallas_call(
            functools.partial(kernel, S, T, chunks, pieces),
            out_shape=jax.ShapeDtypeStruct((rows, width), BF16),
            in_specs=[hbm] * 13,
            out_specs=hbm,
            scratch_shapes=[
                like(tokens),
                like(dq),
                like(dl),
                pltpu.VMEM(dr.shape[::-1], dr.dtype),
                like(uq),
                like(ur),
                like(uk),
                like(uv),
                like(ow),
                pltpu.VMEM((O * span, rank + LANES), BF16),
                pltpu.VMEM((span, dq.shape[1]), BF16),
                pltpu.VMEM((heads, span, NOPE + LANES), BF16),
                pltpu.VMEM((heads, VDIM + 16, span), F32),
                pltpu.VMEM((heads, 8, span), F32),
                pltpu.VMEM((span, heads * VDIM), BF16),
                pltpu.VMEM((2, pieces, rows, width // pieces), BF16),
                pltpu.VMEM((2, pieces, rows, width // pieces), BF16),
                pltpu.VMEM((2, pieces, rows, width // pieces), F32),
                pltpu.VMEM((pieces, rows, width // pieces), BF16),
                pltpu.VMEM((pieces, rows, width // pieces), BF16),
                pltpu.VMEM(uv.shape[::-1], BF16),
                pltpu.VMEM((O // 2, span, heads * NOPE + LANES), BF16),
                pltpu.VMEM((O // 2, heads * VDIM, span), BF16),
                pltpu.VMEM((O // 2, span, heads * NOPE + LANES), BF16),
                pltpu.VMEM((O // 2, heads * VDIM, span), BF16),
                pltpu.VMEM((O, span, heads * NOPE + LANES), BF16),
                pltpu.VMEM((O, heads * VDIM, span), BF16),
                pltpu.VMEM((heads, 2 * span, span), F32),
                pltpu.VMEM((heads, 2 * span, span), F32),
                pltpu.VMEM((heads, 8, span), F32),
                pltpu.VMEM((heads, 8, span), F32),
                pltpu.VMEM((span, LANES), F32),
                pltpu.VMEM((span, LANES), F32),
                pltpu.VMEM((rows, width), BF16),
                pltpu.VMEM((1, dq.shape[1]), F32),
                pltpu.VMEM((1, rank), F32),
                pltpu.VMEM(tables[0].shape, F32),
                pltpu.VMEM(tables[1].shape, F32),
                dma(2 * chunks + 13),
                dma(1),
                dma(1),
                dma(4),
                dma(1),
                dma(T * O),
                dma(2),
                dma(2 * O),
                dma(1),
                dma(4),
                dma(1),
                dma(2 * pieces),
                dma(1),
                dma(pieces),
            ],
            compiler_params=pltpu.CompilerParams(
                collective_id=0, has_side_effects=True, vmem_limit_bytes=63 * 1024 * 1024
            ),
        )(
            tokens, dq, dl, dr.T, qg.reshape(1, -1), lg.reshape(1, -1),
            uq, ur, uk, uv, ow, *tables,
        )
        return total

    return jax.shard_map(
        local,
        mesh=mesh,
        in_specs=(
            P(("sp", "tp"), None),
            P(),
            P(),
            P(),
            P(),
            P(),
            P(None, "tp"),
            P(None, "tp"),
            P(None, "tp"),
            P(None, "tp"),
            P("tp", None),
        ),
        out_specs=P(("sp", "tp"), None),
        check_vma=False,
    )
```

```python
import functools

import jax
import jax.numpy as jnp
import numpy as np
from jax import lax
from jax.experimental import pallas as pl
from jax.experimental.pallas import tpu as pltpu
from jax.sharding import PartitionSpec as P

NOPE = 128
ROPE = 64
VDIM = 128
LANES = 128

rope_base = 500000.0
norm_eps = 1e-06
masked_score = -1e30
log2e = 1.4426950408889634

EVENTS = [
    (0, 0), (3, 0), (1, 0), (0, 3), (0, 1), (3, 3), (1, 3), (3, 1),
    (1, 1), (2, 0), (0, 2), (2, 3), (2, 1), (3, 2), (1, 2), (2, 2),
]
FAR = 9
NEXT = (11, 12)
PASS = {3: (11,), 4: (12,), 7: (15,)}
START = {3: (15,)}
SENT = 60
LEAD = 4
SENT_HALVES = 30

MESH = pl.DeviceIdType.MESH
F32 = jnp.float32
BF16 = jnp.bfloat16


def dot(a, b):
    return jnp.dot(a, b, preferred_element_type=F32)


def dot_nt(a, b):
    return lax.dot_general(a, b, (((1,), (1,)), ((), ())), preferred_element_type=F32)


def turn(v, cosine, sine):
    lane = lax.broadcasted_iota(jnp.int32, v.shape, 1)
    other = jnp.where(lane % ROPE < ROPE // 2, pltpu.roll(v, LANES - ROPE // 2, 1), pltpu.roll(v, ROPE // 2, 1))
    return v * cosine + other * sine


def normed(v, gain):
    return v * lax.rsqrt(jnp.mean(v * v, axis=-1, keepdims=True) + norm_eps) * gain


def kernel(
    S,
    T,
    chunks,
    pieces,
    tokens_hbm,
    dq_hbm,
    dl_hbm,
    dr_hbm,
    qg_hbm,
    lg_hbm,
    uq_hbm,
    ur_hbm,
    uk_hbm,
    uv_hbm,
    ow_hbm,
    base_hbm,
    turn_hbm,
    out_ref,
    tokens,
    dq,
    dl,
    dr,
    uq,
    ur,
    uk,
    uv,
    ow,
    kv,
    ql,
    qh,
    acc,
    best,
    att,
    side_out,
    side_in,
    kept,
    pass_out,
    pass_in,
    uvt,
    keys_a,
    values_a,
    keys_b,
    values_b,
    keys_in,
    values_in,
    scores_a,
    scores_b,
    best_a,
    best_b,
    cos_ref,
    sin_ref,
    qg_ref,
    lg_ref,
    base,
    turns,
    load_sem,
    line_send,
    line_recv,
    kv_send,
    kv_recv,
    share_send,
    share_recv,
    q_send,
    q_recv,
    side_send,
    side_recv,
    pass_send,
    pass_recv,
):
    O = S // 2
    rows = tokens.shape[0]
    span = rows * T
    depth = tokens.shape[1]
    heads = qh.shape[0]
    rank = dl.shape[1]
    sp = lax.axis_index("sp")
    tp = lax.axis_index("tp")
    o, i = sp // 2, sp % 2
    Y = int(O**0.5)
    z, y = o // Y, o % Y
    beside = {"sp": o * 2 + 1 - i, "tp": tp}

    step = depth // chunks
    loads = []

    def load(src, dst):
        copy = pltpu.make_async_copy(src, dst, load_sem.at[len(loads)])
        loads.append(copy)
        copy.start()
        return copy

    tok_load = load(tokens_hbm, tokens)
    small_loads = [load(lg_hbm, lg_ref), load(base_hbm, base), load(turn_hbm, turns), load(qg_hbm, qg_ref)]
    dl_loads = [load(dl_hbm.at[pl.ds(k * step, step)], dl.at[pl.ds(k * step, step)]) for k in range(chunks)]
    dr_load = load(dr_hbm, dr)
    dq_loads = [load(dq_hbm.at[pl.ds(k * step, step)], dq.at[pl.ds(k * step, step)]) for k in range(chunks)]
    barrier = pltpu.get_barrier_semaphore()
    for step_ in (1, Y - 1):
        for node_ in (z * Y + (y + step_) % Y, (z + step_) % Y * Y + y):
            pl.semaphore_signal(barrier, inc=1, device_id={"sp": node_ * 2 + i, "tp": tp}, device_id_type=MESH)
    for n in range(1, T):
        pl.semaphore_signal(barrier, inc=1, device_id={"sp": sp, "tp": (tp + n) % T}, device_id_type=MESH)
    pl.semaphore_signal(barrier, inc=1, device_id=beside, device_id_type=MESH)

    def block_rows(b):
        return pl.ds(pl.multiple_of(b * rows, rows), rows)

    mine = block_rows(o * T + tp)
    first_pos = jnp.where(i == 0, y, z)
    second_pos = jnp.where(i == 0, z, y)

    def node(da, db, i_):
        a_ = (jnp.where(i_ == 0, y, z) + da) % Y
        b_ = (jnp.where(i_ == 0, z, y) + db) % Y
        return jnp.where(i_ == 0, b_ * Y + a_, a_ * Y + b_)

    def send(part, target, send_sem, recv_sem):
        return pltpu.make_async_remote_copy(
            src_ref=part,
            dst_ref=part,
            send_sem=send_sem,
            recv_sem=recv_sem,
            device_id=target,
            device_id_type=MESH,
        )

    def near(t):
        return {"sp": o * 2 + i, "tp": t}

    def ring(da, db):
        return {"sp": node(da, db, i) * 2 + i, "tp": tp}

    def line_part(ref, first, t, h):
        size = rows if h is None else rows // 2
        start_ = first + t * rows + (0 if h is None else h * size)
        return ref.at[pl.ds(pl.multiple_of(start_, size), size)]

    def around(ref, first, send_sem, recv_sem):
        ways = (1, T - 1)

        def own(n):
            part = line_part(ref, first, tp, None)
            send(part, near((tp + ways[n]) % T), send_sem.at[0], recv_sem.at[n]).start()

        def relay_on(n):
            part = line_part(ref, first, (tp + T - ways[n]) % T, n)
            send(part, near((tp + ways[n]) % T), send_sem.at[0], recv_sem.at[2 + n]).start()

        def close_wait(n):
            t = (tp + T - ways[n]) % T
            send(line_part(ref, first, t, None), near(t), send_sem.at[0], recv_sem.at[n]).wait_recv()

        def far_wait(n):
            t = (tp + T // 2) % T
            send(line_part(ref, first, t, n), near(t), send_sem.at[0], recv_sem.at[2 + n]).wait_recv()

        return own, relay_on, close_wait, far_wait

    kv_line = around(kv, o * span, line_send, line_recv)
    q_line = around(ql, 0, q_send, q_recv)

    def sub_copy(n, t, target):
        part = kv.at[block_rows(n * T + t)]
        return send(part, target, kv_send.at[0], kv_recv.at[n * T + t])

    def sub_wait(n, t):
        sub_copy(n, t, beside).wait_recv()

    def steps(k):
        return EVENTS[k]

    def beyond(j):
        return (tp + j) % T

    def first_ring(t):
        for way in (1, Y - 1):
            sub_copy(o, t, ring(way, 0)).start()

    def second_ring(n, t):
        for way in (1, Y - 1):
            sub_copy(n, t, ring(0, way)).start()

    def place(k):
        da, db = steps(k)
        return da, db, node(da, db, i)

    def early(k):
        da, db, n = place(k)
        sub_wait(n, tp)
        second_ring(n, tp)
        pl.when(i == (0 if da == Y - 1 else 1))(sub_copy(n, tp, ring((Y - da) % Y, 0)).start)

    def rest(k):
        n = place(k)[2]
        for j in (1, 3, 2):
            sub_wait(n, beyond(j))
            second_ring(n, beyond(j))

    def whole(k):
        da, db, n = place(k)
        for j in (0, 1, 3, 2):
            sub_wait(n, beyond(j))
            way = Y - 1 if j in (3, 2) else 1
            if db == Y - way:
                sub_copy(n, beyond(j), ring(0, way)).start()

    def cross_start(k):
        da, db, n = place(k)
        sub_wait(n, tp)
        if db == 0:
            second_ring(n, tp)
        if db in (1, Y - 1):
            pl.when(i == (0 if db == Y - 1 else 1))(sub_copy(n, tp, ring(0, Y - db)).start)
        for way in (1, T - 1):
            sub_copy(n, tp, near(beyond(way))).start()

    def cross_pass(k):
        da, db, n = place(k)
        for way in (1, T - 1):
            sub_wait(n, beyond(T - way))
        way = jnp.where((db + i) % 2 == 0, 1, T - 1)
        sub_copy(n, (tp + T - way) % T, near((tp + way) % T)).start()

    def cross_end(k):
        sub_wait(place(k)[2], beyond(2))

    def needs(k):
        da, db, n = place(k)
        return n < o, node(da, db, 1 - i) < o

    def is_late(k):
        da, db = steps(k)
        return da == Y // 2 or (k >= LEAD and db == Y // 2)

    def finish(k):
        cross_end(k) if steps(k)[0] == Y // 2 else whole(k)

    tok_load.wait()
    latent = jnp.zeros((rows, rank), F32)
    for k in range(chunks):
        dl_loads[k].wait()
        latent += dot(tokens[:, k * step : (k + 1) * step], dl[k * step : (k + 1) * step, :])
    dr_load.wait()
    for copy in small_loads:
        copy.wait()
    start_cos, start_sin = base[0, pl.ds(sp, 1), :], base[1, pl.ds(sp, 1), :]
    sign = jnp.where(lax.broadcasted_iota(jnp.int32, (1, LANES), 1) % ROPE < ROPE // 2, -1.0, 1.0)
    cos_ref[...] = start_cos * turns[0] - start_sin * turns[1]
    sin_ref[...] = (start_sin * turns[0] + start_cos * turns[1]) * sign
    turned = dot_nt(tokens[...], dr[...])
    turned = jnp.concatenate([turned, jnp.zeros((rows, LANES - ROPE), F32)], axis=1)
    own_rows = pl.ds(pl.multiple_of(tp * rows, rows), rows)
    kv[mine, :rank] = normed(latent, lg_ref[...]).astype(BF16)
    kv[mine, rank:] = turn(turned, cos_ref[own_rows, :], sin_ref[own_rows, :]).astype(BF16)

    up_loads = [load(uq_hbm, uq), load(ur_hbm, ur), load(uk_hbm, uk), load(uv_hbm, uv)]
    ow_load = load(ow_hbm, ow)
    pl.semaphore_wait(barrier, 4 + T - 1 + 1)
    for n in range(2):
        kv_line[0](n)
    first_ring(tp)
    second_ring(o, tp)

    query = jnp.zeros((rows, dq.shape[1]), F32)
    for k in range(chunks):
        dq_loads[k].wait()
        query += dot(tokens[:, k * step : (k + 1) * step], dq[k * step : (k + 1) * step, :])
    ql[own_rows, :] = normed(query, qg_ref[...]).astype(BF16)

    early(1)
    early(2)
    for n in range(2):
        kv_line[2](n)
        kv_line[1](n)
    for n in range(2):
        q_line[0](n)
    for j in (1, 3):
        first_ring(beyond(j))
        second_ring(o, beyond(j))
    for n in range(2):
        kv_line[3](n)
    first_ring(beyond(2))
    second_ring(o, beyond(2))

    def spot(k):
        n = place(k)[2]
        n = jnp.where(needs(k)[0], n, o) if k >= LEAD else n
        return pl.ds(pl.multiple_of(n * span, span), span)

    def project_keys(k, parity):
        keys = own_keys[parity]
        keys[k // 2, :, : heads * NOPE] = dot(kv[spot(k), :rank], uk[...]).astype(BF16)
        keys[k // 2, :, heads * NOPE :] = kv[spot(k), rank:]

    def project_values(k, parity):
        own_values[parity][k // 2] = dot_nt(uvt[...], kv[spot(k), :rank]).astype(BF16)

    own_keys, own_values = (keys_a, keys_b), (values_a, values_b)
    kept_scores, kept_best = (scores_a, scores_b), (best_a, best_b)

    def share(n, k, parity):
        own, into = ((own_keys, keys_in), (own_values, values_in))[n]
        return pltpu.make_async_remote_copy(
            src_ref=own[parity].at[k // 2],
            dst_ref=into.at[k],
            send_sem=share_send.at[n],
            recv_sem=share_recv.at[n * O + k],
            device_id=beside,
            device_id_type=MESH,
        )

    def prepare_keys(k):
        project_keys(k, k % 2)
        share(0, k, k % 2).start()

    def prepare_values(k):
        project_values(k, k % 2)
        share(1, k, k % 2).start()

    up_loads[2].wait()
    up_loads[3].wait()
    uvt[...] = uv[...].T
    prepare_keys(0)
    prepare_values(0)
    cross_start(FAR)
    for n in range(2):
        q_line[2](n)
        q_line[1](n)
    rest(1)
    rest(2)
    prepare_keys(1)
    prepare_values(1)
    for n in range(2):
        q_line[3](n)
    for copy in up_loads[:2]:
        copy.wait()
    scale = (NOPE + ROPE) ** (-0.5) * log2e
    plain = (dot(ql[...], uq[...]) * scale).astype(BF16)
    turning = dot(ql[...], ur[...]) * scale
    low = lax.broadcasted_iota(jnp.int32, (span, LANES), 1) < ROPE
    for pair in range(heads // 2):
        both = turn(turning[:, pair * LANES : (pair + 1) * LANES], cos_ref[...], sin_ref[...])
        qh[2 * pair, :, NOPE:] = jnp.where(low, both, 0.0).astype(BF16)
        qh[2 * pair + 1, :, NOPE:] = jnp.where(low, pltpu.roll(both, ROPE, 1), 0.0).astype(BF16)
    for h in range(heads):
        qh[h, :, :NOPE] = plain[:, h * NOPE : (h + 1) * NOPE]
        best[h] = jnp.full(best.shape[1:], masked_score, F32)
        acc[h] = jnp.zeros(acc.shape[1:], F32)

    def used(k):
        return (sp >= 0, i == 1) if k == 0 else needs(k)

    def slots(k):
        mine_, other_ = used(k)
        return (jnp.where(mine_, k // 2, 0), jnp.where(other_, k, 0)) if k >= LEAD - 1 else (k // 2, k)

    def score(k, parity, h, masked=False):
        keys = own_keys[parity]
        part = slice(h * NOPE, (h + 1) * NOPE)
        own_, in_ = slots(k)
        rot = jnp.concatenate([keys[own_, :, heads * NOPE :], keys_in[in_, :, heads * NOPE :]], axis=0)
        key = jnp.concatenate([keys[own_, :, part], keys_in[in_, :, part]], axis=0)
        scores = dot_nt(jnp.concatenate([key, rot], axis=1), qh[h])
        pieces_ = [scores[:span], scores[span:]]
        if masked:
            k_pos = lax.broadcasted_iota(jnp.int32, (span, span), 0)
            q_pos = lax.broadcasted_iota(jnp.int32, (span, span), 1)
            pieces_[0] = jnp.where(k_pos <= q_pos, pieces_[0], masked_score)
        top = None
        for n, (piece, use) in enumerate(zip(pieces_, used(k))):
            kept_scores[parity][h, n * span : (n + 1) * span, :] = piece
            limit = jnp.where(use, -masked_score, masked_score)
            new = jnp.minimum(jnp.max(piece, axis=0, keepdims=True), limit)
            top = new if top is None else jnp.maximum(top, new)
        kept_best[parity][h] = jnp.broadcast_to(top, best.shape[1:])

    ones = jnp.ones((acc.shape[1] - VDIM, 2 * span), BF16)

    def weigh(k, parity, h):
        part = slice(h * VDIM, (h + 1) * VDIM)
        own_, in_ = slots(k)
        value = jnp.concatenate([own_values[parity][own_, part, :], values_in[in_, part, :]], axis=1)
        value = jnp.concatenate([value, ones], axis=0)
        old = best[h][:1]
        new = jnp.maximum(old, kept_best[parity][h][:1])
        weights = []
        for n, use in enumerate(used(k)):
            shift = new + jnp.where(use, 0.0, -masked_score)
            weights.append(jnp.exp2(kept_scores[parity][h, n * span : (n + 1) * span, :] - shift).astype(BF16))
        acc[h] = acc[h] * jnp.exp2(old - new) + dot(value, jnp.concatenate(weights, axis=0))
        best[h] = jnp.broadcast_to(new, best.shape[1:])

    count = len(EVENTS)

    def when(condition, act):
        pl.when(condition)(act)

    def step(k):
        parity = k % 2
        scoring, keying, valuing = k + 1 < count, k + LEAD < count, k + LEAD - 1 < count
        wants = [needs(k + LEAD)[0] if keying else None, needs(k + LEAD - 1)[0] if valuing else None]
        if keying:
            if is_late(k + LEAD):
                when(wants[0], lambda: finish(k + LEAD))
            else:
                finish(k + LEAD)
            for table, act in ((PASS, cross_pass), (START, cross_start)):
                for e in table.get(k, ()):
                    act(e)
        if scoring:
            if k + 1 < LEAD:
                share(0, k + 1, 1 - parity).wait_recv()
            else:
                when(needs(k + 1)[1], share(0, k + 1, 1 - parity).wait_recv)
        if k < LEAD - 1:
            share(1, k, parity).wait_recv()
        else:
            when(needs(k)[1], share(1, k, parity).wait_recv)
        needed = used(k)[0] | used(k)[1]
        if scoring:
            needed = needed | used(k + 1)[0] | used(k + 1)[1]

        @pl.when(needed)
        def _():
            for h in range(heads):
                if scoring:
                    score(k + 1, 1 - parity, h)
                if keying and h == 0:
                    project_keys(k + LEAD, parity)
                if valuing and h == 2:
                    project_values(k + LEAD - 1, 1 - parity)
                weigh(k, parity, h)

        spare = [~needed & want for want in wants if want is not None]
        if keying:
            when(spare[0], lambda: project_keys(k + LEAD, parity))
        if valuing:
            when(spare[-1], lambda: project_values(k + LEAD - 1, 1 - parity))
        if keying:
            when(wants[0], share(0, k + LEAD, parity).start)
        if valuing:
            when(wants[1], share(1, k + LEAD - 1, 1 - parity).start)

    cross_pass(FAR)
    for k in NEXT:
        cross_start(k)
    whole(3)
    share(0, 0, 0).wait_recv()
    for h in range(heads):
        score(0, 0, h, masked=True)
    prepare_keys(2)
    prepare_values(2)
    prepare_keys(3)
    for k in range(count - LEAD):
        step(k)
    for k in range(count - LEAD, count):
        step(k)

    for h in range(heads):
        summed = acc[h]
        att[:, h * VDIM : (h + 1) * VDIM] = (summed[:VDIM] / summed[VDIM : VDIM + 1]).T.astype(BF16)

    ow_load.wait()
    width = ow.shape[1] // pieces
    opposite, right, left = (tp + 2) % T, (tp + 1) % T, (tp + T - 1) % T

    def exchange(out, into, target, send_sem, recv_sem):
        return pltpu.make_async_remote_copy(
            src_ref=out,
            dst_ref=into,
            send_sem=send_sem,
            recv_sem=recv_sem,
            device_id=near(target),
            device_id_type=MESH,
        )

    def pass_copy(j):
        target = right if j < pieces // 2 else left
        return exchange(pass_out.at[j], pass_in.at[j], target, pass_send.at[0], pass_recv.at[j])

    def side_copy(side, j):
        n = side * pieces + j
        target = (right, left)[side]
        return exchange(side_out.at[side, j], side_in.at[side, j], target, side_send.at[0], side_recv.at[n])

    attended = jnp.concatenate([att[block_rows(t), :] for t in (opposite, right, left, tp)], axis=0)
    for n in range(pieces):
        j = n // 2 + n % 2 * (pieces // 2)
        late = 0 if j < pieces // 2 else 1
        part = dot(attended, ow[:, j * width : (j + 1) * width])
        pass_out[j] = part[:rows].astype(BF16)
        pass_copy(j).start()
        kept[0, j] = part[(1 + late) * rows : (2 + late) * rows]
        side_out[1 - late, j] = part[(2 - late) * rows : (3 - late) * rows].astype(BF16)
        kept[1, j] = part[3 * rows :]
    order = [n // 2 + n % 2 * (pieces // 2) for n in range(pieces)]
    for j in order:
        late = 0 if j < pieces // 2 else 1
        side_copy(1 - late, j).start()
    for j in order:
        late = 0 if j < pieces // 2 else 1
        pass_copy(j).wait_recv()
        side_out[late, j] = (kept[0, j] + pass_in[j].astype(F32)).astype(BF16)
        side_copy(late, j).start()

    for j in order:
        side_copy(0, j).wait_recv()
        side_copy(1, j).wait_recv()
        total = kept[1, j] + side_in[0, j].astype(F32) + side_in[1, j].astype(F32)
        out_ref[:, j * width : (j + 1) * width] = total.astype(BF16)

    def all_sent(ref, send_sem):
        send(ref, beside, send_sem.at[0], send_sem.at[0]).wait_send()

    all_sent(kv.at[pl.ds(0, SENT * rows)], kv_send)
    for n, (into, always) in enumerate(((keys_in, LEAD), (values_in, LEAD - 1))):
        shared = always
        for k in range(always, count):
            shared = shared + jnp.where(needs(k)[0], 1, 0)
        for k in range(always, count + 1):
            pl.when(shared == k)(send(into.at[pl.ds(0, k)], beside, share_send.at[n], share_send.at[n]).wait_send)
    for k in range(LEAD, count):
        if is_late(k):
            pl.when(~needs(k)[0])(lambda k=k: finish(k))
    all_sent(kv.at[pl.ds(0, 3 * rows)], line_send)
    all_sent(ql.at[pl.ds(0, 3 * rows)], q_send)
    all_sent(side_out, side_send)
    all_sent(pass_out, pass_send)


def solution(mesh):
    S, T = mesh.shape["sp"], mesh.shape["tp"]
    assert S == 32 and T == 4

    def local(tokens, dq, dl, dr, qg, lg, uq, ur, uk, uv, ow):
        rows, depth = tokens.shape
        span = rows * T
        heads = uk.shape[1] // NOPE
        width = ow.shape[1]
        rank = dl.shape[1]
        chunks, pieces = 4, 8
        inverse = np.float32(rope_base) ** (-np.arange(0, ROPE, 2, dtype=np.float32) / np.float32(ROPE))
        inverse = np.tile(inverse.astype(np.float64), LANES // (ROPE // 2))
        starts = np.arange(S)[:, None] * span * inverse
        steps = np.arange(span)[:, None] * inverse
        tables = [jnp.asarray(np.stack([np.cos(a), np.sin(a)]), F32) for a in (starts, steps)]
        O = S // 2
        hbm = pl.BlockSpec(memory_space=pl.ANY)
        dma = lambda n: pltpu.SemaphoreType.DMA((n,))
        like = lambda a: pltpu.VMEM(a.shape, a.dtype)
        total = pl.pallas_call(
            functools.partial(kernel, S, T, chunks, pieces),
            out_shape=pltpu.VMEM((rows, width), BF16),
            in_specs=[hbm] * 13,
            out_specs=pl.BlockSpec(memory_space=pltpu.VMEM),
            scratch_shapes=[
                like(tokens),
                like(dq),
                like(dl),
                pltpu.VMEM(dr.shape[::-1], dr.dtype),
                like(uq),
                like(ur),
                like(uk),
                like(uv),
                like(ow),
                pltpu.VMEM((O * span, rank + LANES), BF16),
                pltpu.VMEM((span, dq.shape[1]), BF16),
                pltpu.VMEM((heads, span, NOPE + LANES), BF16),
                pltpu.VMEM((heads, VDIM + 16, span), F32),
                pltpu.VMEM((heads, 8, span), F32),
                pltpu.VMEM((span, heads * VDIM), BF16),
                pltpu.VMEM((2, pieces, rows, width // pieces), BF16),
                pltpu.VMEM((2, pieces, rows, width // pieces), BF16),
                pltpu.VMEM((2, pieces, rows, width // pieces), F32),
                pltpu.VMEM((pieces, rows, width // pieces), BF16),
                pltpu.VMEM((pieces, rows, width // pieces), BF16),
                pltpu.VMEM(uv.shape[::-1], BF16),
                pltpu.VMEM((O // 2, span, heads * NOPE + LANES), BF16),
                pltpu.VMEM((O // 2, heads * VDIM, span), BF16),
                pltpu.VMEM((O // 2, span, heads * NOPE + LANES), BF16),
                pltpu.VMEM((O // 2, heads * VDIM, span), BF16),
                pltpu.VMEM((O, span, heads * NOPE + LANES), BF16),
                pltpu.VMEM((O, heads * VDIM, span), BF16),
                pltpu.VMEM((heads, 2 * span, span), F32),
                pltpu.VMEM((heads, 2 * span, span), F32),
                pltpu.VMEM((heads, 8, span), F32),
                pltpu.VMEM((heads, 8, span), F32),
                pltpu.VMEM((span, LANES), F32),
                pltpu.VMEM((span, LANES), F32),
                pltpu.VMEM((1, dq.shape[1]), F32),
                pltpu.VMEM((1, rank), F32),
                pltpu.VMEM(tables[0].shape, F32),
                pltpu.VMEM(tables[1].shape, F32),
                dma(2 * chunks + 13),
                dma(1),
                dma(4),
                dma(1),
                dma(T * O),
                dma(2),
                dma(2 * O),
                dma(1),
                dma(4),
                dma(1),
                dma(2 * pieces),
                dma(1),
                dma(pieces),
            ],
            compiler_params=pltpu.CompilerParams(
                collective_id=0, has_side_effects=True, vmem_limit_bytes=63 * 1024 * 1024
            ),
        )(
            tokens, dq, dl, dr.T, qg.reshape(1, -1), lg.reshape(1, -1),
            uq, ur, uk, uv, ow, *tables,
        )
        return total

    return jax.shard_map(
        local,
        mesh=mesh,
        in_specs=(
            P(("sp", "tp"), None),
            P(),
            P(),
            P(),
            P(),
            P(),
            P(None, "tp"),
            P(None, "tp"),
            P(None, "tp"),
            P(None, "tp"),
            P("tp", None),
        ),
        out_specs=P(("sp", "tp"), None),
        check_vma=False,
    )
```

```python
import functools

import jax
import jax.numpy as jnp
import numpy as np
from jax import lax
from jax.experimental import pallas as pl
from jax.experimental.pallas import tpu as pltpu
from jax.sharding import PartitionSpec as P

NOPE = 128
ROPE = 64
VDIM = 128
LANES = 128

rope_base = 500000.0
norm_eps = 1e-06
masked_score = -1e30
log2e = 1.4426950408889634

EVENTS = [
    (0, 0), (3, 0), (1, 0), (0, 3), (0, 1), (3, 3), (1, 3), (3, 1),
    (1, 1), (2, 0), (0, 2), (2, 3), (2, 1), (3, 2), (1, 2), (2, 2),
]
FAR = 9
NEXT = (11, 12)
PASS = {3: (11,), 4: (12,), 7: (15,)}
START = {3: (15,)}
SENT = 60
LEAD = 4
SENT_HALVES = 30

MESH = pl.DeviceIdType.MESH
F32 = jnp.float32
BF16 = jnp.bfloat16


def dot(a, b):
    return jnp.dot(a, b, preferred_element_type=F32)


def dot_nt(a, b):
    return lax.dot_general(a, b, (((1,), (1,)), ((), ())), preferred_element_type=F32)


def turn(v, cosine, sine):
    lane = lax.broadcasted_iota(jnp.int32, v.shape, 1)
    other = jnp.where(lane % ROPE < ROPE // 2, pltpu.roll(v, LANES - ROPE // 2, 1), pltpu.roll(v, ROPE // 2, 1))
    return v * cosine + other * sine


def normed(v, gain):
    return v * lax.rsqrt(jnp.mean(v * v, axis=-1, keepdims=True) + norm_eps) * gain


def kernel(
    S,
    T,
    chunks,
    pieces,
    tokens_hbm,
    dq_hbm,
    dl_hbm,
    dr_hbm,
    qg_hbm,
    lg_hbm,
    uq_hbm,
    ur_hbm,
    uk_hbm,
    uv_hbm,
    ow_hbm,
    base_hbm,
    turn_hbm,
    out_ref,
    tokens,
    dq,
    dl,
    dr,
    uq,
    ur,
    uk,
    uv,
    ow,
    kv,
    ql,
    qh,
    acc,
    best,
    att,
    side_out,
    side_in,
    kept,
    pass_out,
    pass_in,
    uvt,
    keys_a,
    values_a,
    keys_b,
    values_b,
    keys_in,
    values_in,
    scores_a,
    scores_b,
    best_a,
    best_b,
    cos_ref,
    sin_ref,
    qg_ref,
    lg_ref,
    base,
    turns,
    load_sem,
    line_send,
    line_recv,
    kv_send,
    kv_recv,
    share_send,
    share_recv,
    q_send,
    q_recv,
    side_send,
    side_recv,
    pass_send,
    pass_recv,
):
    O = S // 2
    rows = tokens.shape[0]
    span = rows * T
    depth = tokens.shape[1]
    heads = qh.shape[0]
    rank = dl.shape[1]
    sp = lax.axis_index("sp")
    tp = lax.axis_index("tp")
    o, i = sp // 2, sp % 2
    Y = int(O**0.5)
    z, y = o // Y, o % Y
    beside = {"sp": o * 2 + 1 - i, "tp": tp}

    step = depth // chunks
    loads = []

    def load(src, dst):
        copy = pltpu.make_async_copy(src, dst, load_sem.at[len(loads)])
        loads.append(copy)
        copy.start()
        return copy

    tok_load = load(tokens_hbm, tokens)
    small_loads = [load(lg_hbm, lg_ref), load(base_hbm, base), load(turn_hbm, turns), load(qg_hbm, qg_ref)]
    dl_loads = [load(dl_hbm.at[pl.ds(k * step, step)], dl.at[pl.ds(k * step, step)]) for k in range(chunks)]
    dr_load = load(dr_hbm, dr)
    dq_loads = [load(dq_hbm.at[pl.ds(k * step, step)], dq.at[pl.ds(k * step, step)]) for k in range(chunks)]
    barrier = pltpu.get_barrier_semaphore()
    for step_ in (1, Y - 1):
        for node_ in (z * Y + (y + step_) % Y, (z + step_) % Y * Y + y):
            pl.semaphore_signal(barrier, inc=1, device_id={"sp": node_ * 2 + i, "tp": tp}, device_id_type=MESH)
    for n in range(1, T):
        pl.semaphore_signal(barrier, inc=1, device_id={"sp": sp, "tp": (tp + n) % T}, device_id_type=MESH)
    pl.semaphore_signal(barrier, inc=1, device_id=beside, device_id_type=MESH)

    def block_rows(b):
        return pl.ds(pl.multiple_of(b * rows, rows), rows)

    mine = block_rows(o * T + tp)
    first_pos = jnp.where(i == 0, y, z)
    second_pos = jnp.where(i == 0, z, y)

    def node(da, db, i_):
        a_ = (jnp.where(i_ == 0, y, z) + da) % Y
        b_ = (jnp.where(i_ == 0, z, y) + db) % Y
        return jnp.where(i_ == 0, b_ * Y + a_, a_ * Y + b_)

    def send(part, target, send_sem, recv_sem):
        return pltpu.make_async_remote_copy(
            src_ref=part,
            dst_ref=part,
            send_sem=send_sem,
            recv_sem=recv_sem,
            device_id=target,
            device_id_type=MESH,
        )

    def near(t):
        return {"sp": o * 2 + i, "tp": t}

    def ring(da, db):
        return {"sp": node(da, db, i) * 2 + i, "tp": tp}

    def line_part(ref, first, t, h):
        size = rows if h is None else rows // 2
        start_ = first + t * rows + (0 if h is None else h * size)
        return ref.at[pl.ds(pl.multiple_of(start_, size), size)]

    def around(ref, first, send_sem, recv_sem):
        ways = (1, T - 1)

        def own(n):
            part = line_part(ref, first, tp, None)
            send(part, near((tp + ways[n]) % T), send_sem.at[0], recv_sem.at[n]).start()

        def relay_on(n):
            part = line_part(ref, first, (tp + T - ways[n]) % T, n)
            send(part, near((tp + ways[n]) % T), send_sem.at[0], recv_sem.at[2 + n]).start()

        def close_wait(n):
            t = (tp + T - ways[n]) % T
            send(line_part(ref, first, t, None), near(t), send_sem.at[0], recv_sem.at[n]).wait_recv()

        def far_wait(n):
            t = (tp + T // 2) % T
            send(line_part(ref, first, t, n), near(t), send_sem.at[0], recv_sem.at[2 + n]).wait_recv()

        return own, relay_on, close_wait, far_wait

    kv_line = around(kv, o * span, line_send, line_recv)
    q_line = around(ql, 0, q_send, q_recv)

    def sub_copy(n, t, target):
        part = kv.at[block_rows(n * T + t)]
        return send(part, target, kv_send.at[0], kv_recv.at[n * T + t])

    def sub_wait(n, t):
        sub_copy(n, t, beside).wait_recv()

    def steps(k):
        return EVENTS[k]

    def beyond(j):
        return (tp + j) % T

    def first_ring(t):
        for way in (1, Y - 1):
            sub_copy(o, t, ring(way, 0)).start()

    def second_ring(n, t):
        for way in (1, Y - 1):
            sub_copy(n, t, ring(0, way)).start()

    def place(k):
        da, db = steps(k)
        return da, db, node(da, db, i)

    def early(k):
        da, db, n = place(k)
        sub_wait(n, tp)
        second_ring(n, tp)
        pl.when(i == (0 if da == Y - 1 else 1))(sub_copy(n, tp, ring((Y - da) % Y, 0)).start)

    def rest(k):
        n = place(k)[2]
        for j in (1, 3, 2):
            sub_wait(n, beyond(j))
            second_ring(n, beyond(j))

    def whole(k):
        da, db, n = place(k)
        for j in (0, 1, 3, 2):
            sub_wait(n, beyond(j))
            way = Y - 1 if j in (3, 2) else 1
            if db == Y - way:
                sub_copy(n, beyond(j), ring(0, way)).start()

    def cross_start(k):
        da, db, n = place(k)
        sub_wait(n, tp)
        if db == 0:
            second_ring(n, tp)
        if db in (1, Y - 1):
            pl.when(i == (0 if db == Y - 1 else 1))(sub_copy(n, tp, ring(0, Y - db)).start)
        for way in (1, T - 1):
            sub_copy(n, tp, near(beyond(way))).start()

    def cross_pass(k):
        da, db, n = place(k)
        for way in (1, T - 1):
            sub_wait(n, beyond(T - way))
        way = jnp.where((db + i) % 2 == 0, 1, T - 1)
        sub_copy(n, (tp + T - way) % T, near((tp + way) % T)).start()

    def cross_end(k):
        sub_wait(place(k)[2], beyond(2))

    def needs(k):
        da, db, n = place(k)
        return n < o, node(da, db, 1 - i) < o

    def is_late(k):
        da, db = steps(k)
        return da == Y // 2 or (k >= LEAD and db == Y // 2)

    def finish(k):
        cross_end(k) if steps(k)[0] == Y // 2 else whole(k)

    tok_load.wait()
    latent = jnp.zeros((rows, rank), F32)
    for k in range(chunks):
        dl_loads[k].wait()
        latent += dot(tokens[:, k * step : (k + 1) * step], dl[k * step : (k + 1) * step, :])
    dr_load.wait()
    for copy in small_loads:
        copy.wait()
    start_cos, start_sin = base[0, pl.ds(sp, 1), :], base[1, pl.ds(sp, 1), :]
    sign = jnp.where(lax.broadcasted_iota(jnp.int32, (1, LANES), 1) % ROPE < ROPE // 2, -1.0, 1.0)
    cos_ref[...] = start_cos * turns[0] - start_sin * turns[1]
    sin_ref[...] = (start_sin * turns[0] + start_cos * turns[1]) * sign
    turned = dot_nt(tokens[...], dr[...])
    turned = jnp.concatenate([turned, jnp.zeros((rows, LANES - ROPE), F32)], axis=1)
    own_rows = pl.ds(pl.multiple_of(tp * rows, rows), rows)
    kv[mine, :rank] = normed(latent, lg_ref[...]).astype(BF16)
    kv[mine, rank:] = turn(turned, cos_ref[own_rows, :], sin_ref[own_rows, :]).astype(BF16)

    up_loads = [load(uq_hbm, uq), load(ur_hbm, ur), load(uk_hbm, uk), load(uv_hbm, uv)]
    ow_load = load(ow_hbm, ow)
    pl.semaphore_wait(barrier, 4 + T - 1 + 1)
    for n in range(2):
        kv_line[0](n)
    first_ring(tp)
    second_ring(o, tp)

    query = jnp.zeros((rows, dq.shape[1]), F32)
    for k in range(chunks):
        dq_loads[k].wait()
        query += dot(tokens[:, k * step : (k + 1) * step], dq[k * step : (k + 1) * step, :])
    ql[own_rows, :] = normed(query, qg_ref[...]).astype(BF16)

    early(1)
    early(2)
    for n in range(2):
        kv_line[2](n)
        kv_line[1](n)
    for n in range(2):
        q_line[0](n)
    for j in (1, 3):
        first_ring(beyond(j))
        second_ring(o, beyond(j))
    for n in range(2):
        kv_line[3](n)
    first_ring(beyond(2))
    second_ring(o, beyond(2))

    def spot(k):
        n = place(k)[2]
        n = jnp.where(needs(k)[0], n, o) if k >= LEAD else n
        return pl.ds(pl.multiple_of(n * span, span), span)

    def project_keys(k, parity):
        keys = own_keys[parity]
        keys[k // 2, :, : heads * NOPE] = dot(kv[spot(k), :rank], uk[...]).astype(BF16)
        keys[k // 2, :, heads * NOPE :] = kv[spot(k), rank:]

    def project_values(k, parity):
        own_values[parity][k // 2] = dot_nt(uvt[...], kv[spot(k), :rank]).astype(BF16)

    own_keys, own_values = (keys_a, keys_b), (values_a, values_b)
    kept_scores, kept_best = (scores_a, scores_b), (best_a, best_b)

    def share(n, k, parity):
        own, into = ((own_keys, keys_in), (own_values, values_in))[n]
        return pltpu.make_async_remote_copy(
            src_ref=own[parity].at[k // 2],
            dst_ref=into.at[k],
            send_sem=share_send.at[n],
            recv_sem=share_recv.at[n * O + k],
            device_id=beside,
            device_id_type=MESH,
        )

    def prepare_keys(k):
        project_keys(k, k % 2)
        share(0, k, k % 2).start()

    def prepare_values(k):
        project_values(k, k % 2)
        share(1, k, k % 2).start()

    up_loads[2].wait()
    up_loads[3].wait()
    uvt[...] = uv[...].T
    prepare_keys(0)
    prepare_values(0)
    cross_start(FAR)
    for n in range(2):
        q_line[2](n)
        q_line[1](n)
    rest(1)
    rest(2)
    prepare_keys(1)
    prepare_values(1)
    for n in range(2):
        q_line[3](n)
    cross_pass(FAR)
    for k in NEXT:
        cross_start(k)
    whole(3)
    for copy in up_loads[:2]:
        copy.wait()
    share(0, 0, 0).wait_recv()
    scale = (NOPE + ROPE) ** (-0.5) * log2e
    plain = (dot(ql[...], uq[...]) * scale).astype(BF16)
    turning = dot(ql[...], ur[...]) * scale
    low = lax.broadcasted_iota(jnp.int32, (span, LANES), 1) < ROPE
    for pair in range(heads // 2):
        both = turn(turning[:, pair * LANES : (pair + 1) * LANES], cos_ref[...], sin_ref[...])
        qh[2 * pair, :, NOPE:] = jnp.where(low, both, 0.0).astype(BF16)
        qh[2 * pair + 1, :, NOPE:] = jnp.where(low, pltpu.roll(both, ROPE, 1), 0.0).astype(BF16)
    for h in range(heads):
        qh[h, :, :NOPE] = plain[:, h * NOPE : (h + 1) * NOPE]
        best[h] = jnp.full(best.shape[1:], masked_score, F32)
        acc[h] = jnp.zeros(acc.shape[1:], F32)
    project_keys(2, 0)
    project_values(2, 0)
    project_keys(3, 1)

    def used(k):
        return (sp >= 0, i == 1) if k == 0 else needs(k)

    def slots(k):
        mine_, other_ = used(k)
        return (jnp.where(mine_, k // 2, 0), jnp.where(other_, k, 0)) if k >= LEAD - 1 else (k // 2, k)

    def score(k, parity, h, masked=False):
        keys = own_keys[parity]
        part = slice(h * NOPE, (h + 1) * NOPE)
        own_, in_ = slots(k)
        rot = jnp.concatenate([keys[own_, :, heads * NOPE :], keys_in[in_, :, heads * NOPE :]], axis=0)
        key = jnp.concatenate([keys[own_, :, part], keys_in[in_, :, part]], axis=0)
        scores = dot_nt(jnp.concatenate([key, rot], axis=1), qh[h])
        pieces_ = [scores[:span], scores[span:]]
        if masked:
            k_pos = lax.broadcasted_iota(jnp.int32, (span, span), 0)
            q_pos = lax.broadcasted_iota(jnp.int32, (span, span), 1)
            pieces_[0] = jnp.where(k_pos <= q_pos, pieces_[0], masked_score)
        top = None
        for n, (piece, use) in enumerate(zip(pieces_, used(k))):
            kept_scores[parity][h, n * span : (n + 1) * span, :] = piece
            limit = jnp.where(use, -masked_score, masked_score)
            new = jnp.minimum(jnp.max(piece, axis=0, keepdims=True), limit)
            top = new if top is None else jnp.maximum(top, new)
        kept_best[parity][h] = jnp.broadcast_to(top, best.shape[1:])

    ones = jnp.ones((acc.shape[1] - VDIM, 2 * span), BF16)

    def weigh(k, parity, h):
        part = slice(h * VDIM, (h + 1) * VDIM)
        own_, in_ = slots(k)
        value = jnp.concatenate([own_values[parity][own_, part, :], values_in[in_, part, :]], axis=1)
        value = jnp.concatenate([value, ones], axis=0)
        old = best[h][:1]
        new = jnp.maximum(old, kept_best[parity][h][:1])
        weights = []
        for n, use in enumerate(used(k)):
            shift = new + jnp.where(use, 0.0, -masked_score)
            weights.append(jnp.exp2(kept_scores[parity][h, n * span : (n + 1) * span, :] - shift).astype(BF16))
        acc[h] = acc[h] * jnp.exp2(old - new) + dot(value, jnp.concatenate(weights, axis=0))
        best[h] = jnp.broadcast_to(new, best.shape[1:])

    count = len(EVENTS)

    def when(condition, act):
        pl.when(condition)(act)

    def step(k):
        parity = k % 2
        scoring, keying, valuing = k + 1 < count, k + LEAD < count, k + LEAD - 1 < count
        wants = [needs(k + LEAD)[0] if keying else None, needs(k + LEAD - 1)[0] if valuing else None]
        if keying:
            if is_late(k + LEAD):
                when(wants[0], lambda: finish(k + LEAD))
            else:
                finish(k + LEAD)
            for table, act in ((PASS, cross_pass), (START, cross_start)):
                for e in table.get(k, ()):
                    act(e)
        if scoring:
            if k + 1 < LEAD:
                share(0, k + 1, 1 - parity).wait_recv()
            else:
                when(needs(k + 1)[1], share(0, k + 1, 1 - parity).wait_recv)
        if k < LEAD - 1:
            share(1, k, parity).wait_recv()
        else:
            when(needs(k)[1], share(1, k, parity).wait_recv)
        needed = used(k)[0] | used(k)[1]
        if scoring:
            needed = needed | used(k + 1)[0] | used(k + 1)[1]

        @pl.when(needed)
        def _():
            for h in range(heads):
                weigh(k, parity, h)
                if keying and h == 0:
                    project_keys(k + LEAD, parity)
                if valuing and h == 2:
                    project_values(k + LEAD - 1, 1 - parity)
                if scoring:
                    score(k + 1, 1 - parity, h)

        spare = [~needed & want for want in wants if want is not None]
        if keying:
            when(spare[0], lambda: project_keys(k + LEAD, parity))
        if valuing:
            when(spare[-1], lambda: project_values(k + LEAD - 1, 1 - parity))
        if keying:
            when(wants[0], share(0, k + LEAD, parity).start)
        if valuing:
            when(wants[1], share(1, k + LEAD - 1, 1 - parity).start)

    for h in range(heads):
        score(0, 0, h, masked=True)
    for copy in (share(0, 2, 0), share(1, 2, 0), share(0, 3, 1)):
        copy.start()
    for k in range(count - LEAD):
        step(k)
    for k in range(count - LEAD, count):
        step(k)

    for h in range(heads):
        summed = acc[h]
        att[:, h * VDIM : (h + 1) * VDIM] = (summed[:VDIM] / summed[VDIM : VDIM + 1]).T.astype(BF16)

    ow_load.wait()
    width = ow.shape[1] // pieces
    opposite, right, left = (tp + 2) % T, (tp + 1) % T, (tp + T - 1) % T

    def exchange(out, into, target, send_sem, recv_sem):
        return pltpu.make_async_remote_copy(
            src_ref=out,
            dst_ref=into,
            send_sem=send_sem,
            recv_sem=recv_sem,
            device_id=near(target),
            device_id_type=MESH,
        )

    def pass_copy(j):
        target = right if j < pieces // 2 else left
        return exchange(pass_out.at[j], pass_in.at[j], target, pass_send.at[0], pass_recv.at[j])

    def side_copy(side, j):
        target = (right, left)[side]
        return exchange(side_out.at[side, j], side_in.at[j, side], target, side_send.at[0], side_recv.at[j])

    attended = jnp.concatenate([att[block_rows(t), :] for t in (opposite, right, left, tp)], axis=0)
    for n in range(pieces):
        j = n // 2 + n % 2 * (pieces // 2)
        late = 0 if j < pieces // 2 else 1
        part = dot(attended, ow[:, j * width : (j + 1) * width])
        pass_out[j] = part[:rows].astype(BF16)
        pass_copy(j).start()
        kept[0, j] = part[(1 + late) * rows : (2 + late) * rows]
        side_out[1 - late, j] = part[(2 - late) * rows : (3 - late) * rows].astype(BF16)
        kept[1, j] = part[3 * rows :]
    order = [n // 2 + n % 2 * (pieces // 2) for n in range(pieces)]
    for j in order:
        late = 0 if j < pieces // 2 else 1
        side_copy(1 - late, j).start()
    for j in order:
        late = 0 if j < pieces // 2 else 1
        pass_copy(j).wait_recv()
        side_out[late, j] = (kept[0, j] + pass_in[j].astype(F32)).astype(BF16)
        side_copy(late, j).start()

    for j in order:
        exchange(side_in.at[j], side_in.at[j], left, side_send.at[0], side_recv.at[j]).wait_recv()
        total = kept[1, j] + side_in[j, 0].astype(F32) + side_in[j, 1].astype(F32)
        out_ref[:, j * width : (j + 1) * width] = total.astype(BF16)

    def all_sent(ref, send_sem):
        send(ref, beside, send_sem.at[0], send_sem.at[0]).wait_send()

    all_sent(kv.at[pl.ds(0, SENT * rows)], kv_send)
    for n, (into, always) in enumerate(((keys_in, LEAD), (values_in, LEAD - 1))):
        shared = always
        for k in range(always, count):
            shared = shared + jnp.where(needs(k)[0], 1, 0)
        for k in range(always, count + 1):
            pl.when(shared == k)(send(into.at[pl.ds(0, k)], beside, share_send.at[n], share_send.at[n]).wait_send)
    for k in range(LEAD, count):
        if is_late(k):
            pl.when(~needs(k)[0])(lambda k=k: finish(k))
    all_sent(kv.at[pl.ds(0, 3 * rows)], line_send)
    all_sent(ql.at[pl.ds(0, 3 * rows)], q_send)
    all_sent(side_out, side_send)
    all_sent(pass_out, pass_send)


def solution(mesh):
    S, T = mesh.shape["sp"], mesh.shape["tp"]
    assert S == 32 and T == 4

    def local(tokens, dq, dl, dr, qg, lg, uq, ur, uk, uv, ow):
        rows, depth = tokens.shape
        span = rows * T
        heads = uk.shape[1] // NOPE
        width = ow.shape[1]
        rank = dl.shape[1]
        chunks, pieces = 4, 8
        inverse = np.float32(rope_base) ** (-np.arange(0, ROPE, 2, dtype=np.float32) / np.float32(ROPE))
        inverse = np.tile(inverse.astype(np.float64), LANES // (ROPE // 2))
        starts = np.arange(S)[:, None] * span * inverse
        steps = np.arange(span)[:, None] * inverse
        tables = [jnp.asarray(np.stack([np.cos(a), np.sin(a)]), F32) for a in (starts, steps)]
        O = S // 2
        hbm = pl.BlockSpec(memory_space=pl.ANY)
        dma = lambda n: pltpu.SemaphoreType.DMA((n,))
        like = lambda a: pltpu.VMEM(a.shape, a.dtype)
        total = pl.pallas_call(
            functools.partial(kernel, S, T, chunks, pieces),
            out_shape=pltpu.VMEM((rows, width), BF16),
            in_specs=[hbm] * 13,
            out_specs=pl.BlockSpec(memory_space=pltpu.VMEM),
            scratch_shapes=[
                like(tokens),
                like(dq),
                like(dl),
                pltpu.VMEM(dr.shape[::-1], dr.dtype),
                like(uq),
                like(ur),
                like(uk),
                like(uv),
                like(ow),
                pltpu.VMEM((O * span, rank + LANES), BF16),
                pltpu.VMEM((span, dq.shape[1]), BF16),
                pltpu.VMEM((heads, span, NOPE + LANES), BF16),
                pltpu.VMEM((heads, VDIM + 16, span), F32),
                pltpu.VMEM((heads, 8, span), F32),
                pltpu.VMEM((span, heads * VDIM), BF16),
                pltpu.VMEM((2, pieces, rows, width // pieces), BF16),
                pltpu.VMEM((pieces, 2, rows, width // pieces), BF16),
                pltpu.VMEM((2, pieces, rows, width // pieces), F32),
                pltpu.VMEM((pieces, rows, width // pieces), BF16),
                pltpu.VMEM((pieces, rows, width // pieces), BF16),
                pltpu.VMEM(uv.shape[::-1], BF16),
                pltpu.VMEM((O // 2, span, heads * NOPE + LANES), BF16),
                pltpu.VMEM((O // 2, heads * VDIM, span), BF16),
                pltpu.VMEM((O // 2, span, heads * NOPE + LANES), BF16),
                pltpu.VMEM((O // 2, heads * VDIM, span), BF16),
                pltpu.VMEM((O, span, heads * NOPE + LANES), BF16),
                pltpu.VMEM((O, heads * VDIM, span), BF16),
                pltpu.VMEM((heads, 2 * span, span), F32),
                pltpu.VMEM((heads, 2 * span, span), F32),
                pltpu.VMEM((heads, 8, span), F32),
                pltpu.VMEM((heads, 8, span), F32),
                pltpu.VMEM((span, LANES), F32),
                pltpu.VMEM((span, LANES), F32),
                pltpu.VMEM((1, dq.shape[1]), F32),
                pltpu.VMEM((1, rank), F32),
                pltpu.VMEM(tables[0].shape, F32),
                pltpu.VMEM(tables[1].shape, F32),
                dma(2 * chunks + 13),
                dma(1),
                dma(4),
                dma(1),
                dma(T * O),
                dma(2),
                dma(2 * O),
                dma(1),
                dma(4),
                dma(1),
                dma(pieces),
                dma(1),
                dma(pieces),
            ],
            compiler_params=pltpu.CompilerParams(
                collective_id=0, has_side_effects=True, vmem_limit_bytes=63 * 1024 * 1024
            ),
        )(
            tokens, dq, dl, dr.T, qg.reshape(1, -1), lg.reshape(1, -1),
            uq, ur, uk, uv, ow, *tables,
        )
        return total

    return jax.shard_map(
        local,
        mesh=mesh,
        in_specs=(
            P(("sp", "tp"), None),
            P(),
            P(),
            P(),
            P(),
            P(),
            P(None, "tp"),
            P(None, "tp"),
            P(None, "tp"),
            P(None, "tp"),
            P("tp", None),
        ),
        out_specs=P(("sp", "tp"), None),
        check_vma=False,
    )
```
